32 devices in a mesh: ep: 8 (over z, core), tp: 4 (over y, x).
Axes of the slice: x: 2, y: 2, z: 4, core: 2. Of those that a mesh axis runs over, the one named last changes fastest.
Arguments:
- stream: bfloat16 [128, 4096], P('ep'), may hold values from -6 to 6
- previous_state: float32 [128, 128, 4096], P('ep', None, 'tp'), may hold values from -6 to 6
- mixer_norm_gain: float32 [4096], replicated, may hold values from 0.1 to 1.9
- query_matrix: bfloat16 [4096, 2048], P('ep'), may hold values from -0.09375 to 0.09375
- key_matrix: bfloat16 [4096, 2048], P('ep'), may hold values from -0.09375 to 0.09375
- value_matrix: bfloat16 [4096, 4096], P('ep', 'tp'), may hold values from -0.09375 to 0.09375
- output_gate_weight: bfloat16 [4096, 4096], P('ep', 'tp'), may hold values from -0.09375 to 0.09375
- decay_lower_factor: bfloat16 [4096, 64], replicated, may hold values from -0.09375 to 0.09375
- decay_upper_factor: bfloat16 [64, 2048], replicated, may hold values from -3 to 3
- forgetting_boost: float32 [128, 2048], P('ep'), may hold values from 0.02 to 1.5
- head_norm_gain: float32 [256], replicated, may hold values from 0.1 to 1.9
- output_matrix: bfloat16 [4096, 4096], P('tp'), may hold values from -0.1875 to 0.1875
- mixture_norm_gain: float32 [4096], replicated, may hold values from 0.1 to 1.9
- expert_gate_weight: bfloat16 [8, 1024, 4096], P('ep', 'tp'), may hold values from -0.09375 to 0.09375
- expert_up_weight: bfloat16 [8, 1024, 4096], P('ep', 'tp'), may hold values from -0.09375 to 0.09375
- expert_down_weight: bfloat16 [8, 1024, 4096], P('ep', None, 'tp'), may hold values from -0.375 to 0.375
- expert_index_table: int32 [128, 2], P('ep'), may hold values from 0 to 7, as said below
- expert_scores_within: float32 [128, 2], P('ep'), may hold values from -6 to 6
- group_probability: float32 [128], P('ep'), may hold values from 0.3 to 1
Outputs:
- new_stream: bfloat16 [128, 4096], P('ep', 'tp')
- new_state: float32 [128, 128, 4096], P('ep', None, 'tp')
The draws below stay inside these ranges and needn't reach their ends.
Inputs may be any that keep to these rules, and one draw needn't show every extreme that they name: `expert_index_table`: the 2 experts of a sequence are distinct and lie in one group of 2 consecutive experts. Among the 16 sequences of one index of ep (aligned blocks of rows), each expert is named at most 8 times, and in every block some experts are named exactly 8 times.
All inputs are finite; a program needn't handle non-finite values.
Results may differ from the reference program's by a relative error of at most 0.02.
Values may be sent and summed in bfloat16 or wider, within the bound.
A program may use at most 128 MiB of HBM per device.

```python
import math
import jax
import jax.numpy as jnp
from jax import lax

D = 4096
HEAD_TOTAL = 16
KEY_CHANNELS = 128
DV = 256
RANK = 64
FF = 1024
GROUPS = 4
TOPK = 2
SEQ_DEV = 16
SEQUENCE_TOTAL = 128
EXPERTS = 8
PER_GROUP = 2
CAP = 8
N_EP = 8


def shuffle(subkey):
    return jax.random.permutation(subkey, SEQ_DEV)


def draw_expert_index_table(key, part):
    blocks = SEQUENCE_TOTAL // SEQ_DEV
    hot_count = PER_GROUP * CAP // TOPK
    key_hot, key_other, key_perm, key_turn = jax.random.split(jax.random.fold_in(key, 11), 4)
    hot_group = jax.random.randint(key_hot, (), 0, GROUPS)
    offsets = jax.random.randint(key_other, (blocks, SEQ_DEV), 1, GROUPS)
    orders = jax.vmap(shuffle)(jax.random.split(key_perm, blocks))
    places = jnp.arange(SEQ_DEV)
    chosen = (orders[:, :, None] == places[None, None, :]) & (places[None, :, None] < hot_count)
    is_hot = jnp.any(chosen, axis=1)
    group_id = jnp.where(is_hot, hot_group, (hot_group + offsets) % GROUPS)
    same_group = group_id[:, :, None] == group_id[:, None, :]
    before = places[None, :] < places[:, None]
    rank_in = jnp.sum(same_group & before[None], axis=2)
    rotation = jax.random.randint(key_turn, (blocks, GROUPS), 0, PER_GROUP)
    member = group_id[:, :, None] == jnp.arange(GROUPS)[None, None, :]
    shift_by = jnp.sum(jnp.where(member, rotation[:, None, :], 0), axis=2)
    within = (shift_by[:, :, None] + rank_in[:, :, None] * TOPK + jnp.arange(TOPK)[None, None, :]) % PER_GROUP
    chosen_ids = group_id[:, :, None] * PER_GROUP + within
    return chosen_ids.reshape(SEQUENCE_TOTAL, TOPK).astype(jnp.int32)


def block_scale(rng, dims, pieces, least, high):
    def one(position, shards_of):
        steps = jax.random.uniform(jax.random.fold_in(jax.random.fold_in(rng, 6), position), (shards_of,), jnp.float32, least / len(pieces), high / len(pieces))
        return jnp.repeat(jnp.exp(steps), dims[position] // shards_of).reshape((-1,) + (1,) * (len(dims) - position - 1))

    level = one(*pieces[0])
    for cut in pieces[1:]:
        level = level * one(*cut)
    return level


def centred(stream_key, dims, width, limit, cuts=(), kind=jnp.bfloat16):
    result = jax.random.normal(stream_key, dims, jnp.float32) * width
    if len(cuts) > 0:
        result = block_scale(stream_key, dims, cuts, -0.22, 0.18) * result
    return jnp.clip(result, min=-limit, max=limit).astype(kind)


def setup_inputs(seed: int = 0) -> dict:
    key_list = jax.random.split(jax.random.key(seed), 20)
    return {
        "stream": centred(key_list[0], (SEQUENCE_TOTAL, D), 1.0, 6.0, ((0, 8),)),
        "previous_state": centred(key_list[1], (SEQUENCE_TOTAL, KEY_CHANNELS, HEAD_TOTAL * DV), 1.0, 6.0, ((0, 8), (2, 4)), jnp.float32),
        "mixer_norm_gain": jnp.clip(1.0 + 0.18 * jax.random.normal(key_list[2], (D,), jnp.float32), 0.1, 1.9),
        "query_matrix": centred(key_list[3], (D, HEAD_TOTAL * KEY_CHANNELS), D ** -0.5, 0.09375, ((0, 8),)),
        "key_matrix": centred(key_list[4], (D, HEAD_TOTAL * KEY_CHANNELS), D ** -0.5, 0.09375, ((0, 8),)),
        "value_matrix": centred(key_list[5], (D, HEAD_TOTAL * DV), D ** -0.5, 0.09375, ((0, 8), (1, 4))),
        "output_gate_weight": centred(key_list[6], (D, HEAD_TOTAL * DV), D ** -0.5, 0.09375, ((0, 8), (1, 4))),
        "decay_lower_factor": centred(key_list[7], (D, RANK), D ** -0.5, 0.09375),
        "decay_upper_factor": centred(key_list[8], (RANK, HEAD_TOTAL * KEY_CHANNELS), (RANK // 16) ** -0.5, 3.0),
        "forgetting_boost": jnp.clip(jnp.exp(math.log(1.5) - 4.317488 * jax.random.uniform(key_list[9], (SEQUENCE_TOTAL, HEAD_TOTAL * KEY_CHANNELS), jnp.float32) ** block_scale(key_list[9], (SEQUENCE_TOTAL, HEAD_TOTAL * KEY_CHANNELS), ((0, 8),), -0.2, 0.2)), 0.02, 1.5),
        "head_norm_gain": jnp.clip(1.0 + 0.18 * jax.random.normal(key_list[10], (DV,), jnp.float32), 0.1, 1.9),
        "output_matrix": centred(key_list[11], (HEAD_TOTAL * DV, D), (HEAD_TOTAL * DV // 4) ** -0.5, 0.1875, ((0, 4),)),
        "mixture_norm_gain": jnp.clip(1.0 + 0.18 * jax.random.normal(key_list[12], (D,), jnp.float32), 0.1, 1.9),
        "expert_gate_weight": centred(key_list[13], (EXPERTS, FF, D), D ** -0.5, 0.09375, ((0, 8), (1, 4))),
        "expert_up_weight": centred(key_list[14], (EXPERTS, FF, D), D ** -0.5, 0.09375, ((0, 8), (1, 4))),
        "expert_down_weight": centred(key_list[15], (EXPERTS, FF, D), (FF // 4) ** -0.5, 0.375, ((0, 8), (2, 4))),
        "expert_index_table": draw_expert_index_table(jax.random.fold_in(key_list[19], 71), 0),
        "expert_scores_within": centred(key_list[17], (SEQUENCE_TOTAL, TOPK), 1.5, 6.0, ((0, 8),), jnp.float32),
        "group_probability": jnp.clip(0.3 + 0.7 * jax.random.uniform(key_list[18], (SEQUENCE_TOTAL,), jnp.float32) ** block_scale(key_list[18], (SEQUENCE_TOTAL,), ((0, 8),), -0.2, 0.2), 0.3, 1.0),
    }


epsilon = 1e-06
forgetting_softness = 16.0

def rms_scaled(values, gain_vec):
    floats = values.astype(jnp.float32)
    scaled = floats * lax.rsqrt(lax.optimization_barrier(jnp.mean(floats * floats, axis=-1, keepdims=True)) + epsilon)
    return (scaled * gain_vec).astype(jnp.bfloat16)

def expert_apply(inputs):
    tokens_in, gate_mat, up_mat, down_mat = inputs
    gate_pre = jnp.dot(tokens_in, gate_mat.T, preferred_element_type=jnp.float32)
    up_pre = jnp.dot(tokens_in, up_mat.T, preferred_element_type=jnp.float32)
    hidden = (jax.nn.silu(gate_pre) * up_pre).astype(jnp.bfloat16)
    return jnp.dot(hidden, down_mat, preferred_element_type=jnp.float32).astype(jnp.bfloat16)

def reference(stream, previous_state, mixer_norm_gain, query_matrix, key_matrix, value_matrix, output_gate_weight, decay_lower_factor, decay_upper_factor, forgetting_boost, head_norm_gain, output_matrix, mixture_norm_gain, expert_gate_weight, expert_up_weight, expert_down_weight, expert_index_table, expert_scores_within, group_probability):
    normed = rms_scaled(stream, mixer_norm_gain)
    queries = (jnp.dot(normed, query_matrix, preferred_element_type=jnp.float32) * KEY_CHANNELS ** (-0.5)).astype(jnp.bfloat16)
    key_rows = jnp.dot(normed, key_matrix, preferred_element_type=jnp.float32).astype(jnp.bfloat16)
    value_rows = jnp.dot(normed, value_matrix, preferred_element_type=jnp.float32).astype(jnp.bfloat16)
    gate_rows = jnp.dot(normed, output_gate_weight, preferred_element_type=jnp.float32).astype(jnp.bfloat16)
    low_rank = jnp.dot(normed, decay_lower_factor, preferred_element_type=jnp.float32).astype(jnp.bfloat16)
    forgetting_logit = jnp.dot(low_rank, decay_upper_factor, preferred_element_type=jnp.float32)
    forgetting_lograte = jax.nn.log_sigmoid(forgetting_logit) / forgetting_softness - forgetting_boost
    factor = jnp.exp(forgetting_lograte).reshape(SEQUENCE_TOTAL, HEAD_TOTAL, KEY_CHANNELS).transpose(0, 2, 1)[..., None]
    state_four = previous_state.reshape(SEQUENCE_TOTAL, KEY_CHANNELS, HEAD_TOTAL, DV)
    key_part = key_rows.astype(jnp.float32).reshape(SEQUENCE_TOTAL, HEAD_TOTAL, KEY_CHANNELS).transpose(0, 2, 1)[..., None]
    value_part = value_rows.astype(jnp.float32).reshape(SEQUENCE_TOTAL, 1, HEAD_TOTAL, DV)
    updated = factor * state_four + key_part * value_part
    query_part = queries.astype(jnp.float32).reshape(SEQUENCE_TOTAL, HEAD_TOTAL, KEY_CHANNELS).transpose(0, 2, 1)
    readout = jnp.einsum('skh,skhv->shv', query_part, updated, precision=lax.Precision.HIGHEST)
    mean_sq = lax.optimization_barrier(jnp.mean(readout * readout, axis=-1, keepdims=True))
    gate_part = jax.nn.silu(gate_rows.astype(jnp.float32).reshape(SEQUENCE_TOTAL, HEAD_TOTAL, DV))
    gated_rows = (readout * lax.rsqrt(mean_sq + epsilon) * head_norm_gain * gate_part).reshape(SEQUENCE_TOTAL, HEAD_TOTAL * DV).astype(jnp.bfloat16)
    blended_tokens = (stream.astype(jnp.float32) + jnp.dot(gated_rows, output_matrix, preferred_element_type=jnp.float32)).astype(jnp.bfloat16)
    normed_two = rms_scaled(blended_tokens, mixture_norm_gain)
    logit_exp = jnp.exp(expert_scores_within)
    weights = logit_exp / lax.optimization_barrier(jnp.sum(logit_exp, axis=-1, keepdims=True)) * group_probability[:, None]
    blocked = expert_index_table.reshape(N_EP, SEQ_DEV * TOPK).astype(jnp.int32)
    one_hot = (blocked[..., None] == jnp.arange(EXPERTS, dtype=jnp.int32)).astype(jnp.int32)
    rank_in = lax.optimization_barrier(jnp.sum(one_hot * (jnp.cumsum(one_hot, axis=1) - 1), axis=-1))
    column = (jnp.arange(N_EP, dtype=jnp.int32)[:, None] * CAP + rank_in).astype(jnp.int32)
    repeated = jnp.broadcast_to(normed_two.reshape(N_EP, SEQ_DEV, 1, D), (N_EP, SEQ_DEV, TOPK, D)).reshape(N_EP, SEQ_DEV * TOPK, D)
    buffer = jnp.zeros((EXPERTS, N_EP * CAP, D), jnp.bfloat16).at[blocked, column].set(repeated)
    results = lax.map(expert_apply, (buffer, expert_gate_weight, expert_up_weight, expert_down_weight))
    picked = results[blocked, column].reshape(SEQUENCE_TOTAL, TOPK, D)
    mixture = lax.optimization_barrier(jnp.sum(weights[..., None] * picked.astype(jnp.float32), axis=1))
    new_stream = (blended_tokens.astype(jnp.float32) + mixture).astype(jnp.bfloat16)
    return (new_stream, updated.reshape(SEQUENCE_TOTAL, KEY_CHANNELS, HEAD_TOTAL * DV))
```

```python
import functools

import jax
import jax.numpy as jnp
from jax import lax
from jax.experimental import pallas as pl
from jax.experimental.pallas import tpu as pltpu
from jax.sharding import PartitionSpec as P

HEAD_TOTAL = 16
KEY_CHANNELS = 128
DV = 256
GROUPS = 4
STEP = 4
COST = 20_000_000_000
VM3 = 10
F32 = jnp.float32
BF16 = jnp.bfloat16
MESH = pl.DeviceIdType.MESH

epsilon = 1e-06
forgetting_softness = 16.0


def rms_scaled(values, gain_vec):
    floats = values.astype(jnp.float32)
    scaled = floats * lax.rsqrt(jnp.mean(floats * floats, axis=-1, keepdims=True) + epsilon)
    return (scaled * gain_vec).astype(jnp.bfloat16)


def general(
    stream,
    previous_state,
    mixer_norm_gain,
    query_matrix,
    key_matrix,
    value_matrix,
    output_gate_weight,
    decay_lower_factor,
    decay_upper_factor,
    forgetting_boost,
    head_norm_gain,
    output_matrix,
    mixture_norm_gain,
    expert_gate_weight,
    expert_up_weight,
    expert_down_weight,
    expert_index_table,
    expert_scores_within,
    group_probability,
):
    seq_count, model_width = stream.shape
    value_local = previous_state.shape[2]
    head_count = max(1, value_local // DV)
    head_width = min(value_local, DV)
    tp_index = lax.axis_index("tp")
    leading_head = tp_index * value_local // DV
    value_start = tp_index * value_local % DV
    key_column_span = head_count * KEY_CHANNELS
    normed = rms_scaled(stream, mixer_norm_gain)
    own_query = lax.dynamic_slice_in_dim(
        query_matrix, leading_head * KEY_CHANNELS, key_column_span, 1
    )
    own_key = lax.dynamic_slice_in_dim(key_matrix, leading_head * KEY_CHANNELS, key_column_span, 1)
    spread = lax.all_to_all(normed, "ep", split_axis=1, concat_axis=0, tiled=True)
    joined = jnp.concatenate([own_query, own_key, value_matrix, output_gate_weight], axis=1)
    summed = lax.psum_scatter(
        jnp.dot(spread, joined, preferred_element_type=jnp.float32),
        "ep",
        scatter_dimension=0,
        tiled=True,
    )
    query_sum = summed[:, :key_column_span]
    key_sum = summed[:, key_column_span : 2 * key_column_span]
    value_sum = summed[:, 2 * key_column_span : 2 * key_column_span + value_local]
    gate_sum = summed[:, 2 * key_column_span + value_local :]
    queries = (query_sum * KEY_CHANNELS ** (-0.5)).astype(jnp.bfloat16)
    key_rows = key_sum.astype(jnp.bfloat16)
    value_rows = value_sum.astype(jnp.bfloat16)
    gate_rows = gate_sum.astype(jnp.bfloat16)
    low_rank = jnp.dot(normed, decay_lower_factor, preferred_element_type=jnp.float32).astype(
        jnp.bfloat16
    )
    local_expand_matrix = lax.dynamic_slice_in_dim(
        decay_upper_factor, leading_head * KEY_CHANNELS, key_column_span, 1
    )
    forgetting_logit = jnp.dot(low_rank, local_expand_matrix, preferred_element_type=jnp.float32)
    request_boost = lax.dynamic_slice_in_dim(
        forgetting_boost, leading_head * KEY_CHANNELS, key_column_span, 1
    )
    forgetting_lograte = jax.nn.log_sigmoid(forgetting_logit) / forgetting_softness - request_boost
    factor = (
        jnp.exp(forgetting_lograte)
        .reshape(seq_count, head_count, KEY_CHANNELS)
        .transpose(0, 2, 1)[..., None]
    )
    state_four = previous_state.reshape(seq_count, KEY_CHANNELS, head_count, head_width)
    key_part = (
        key_rows.astype(jnp.float32)
        .reshape(seq_count, head_count, KEY_CHANNELS)
        .transpose(0, 2, 1)[..., None]
    )
    value_part = value_rows.astype(jnp.float32).reshape(seq_count, 1, head_count, head_width)
    updated = factor * state_four + key_part * value_part
    query_part = (
        queries.astype(jnp.float32).reshape(seq_count, head_count, KEY_CHANNELS).transpose(0, 2, 1)
    )
    readout = jnp.einsum("skh,skhv->shv", query_part, updated, precision=lax.Precision.HIGHEST)
    square_sums = jnp.sum(readout * readout, axis=-1)
    norm_table = lax.dynamic_update_slice(
        jnp.zeros((seq_count, HEAD_TOTAL), jnp.float32), square_sums, (jnp.int32(0), leading_head)
    )
    totals = lax.psum(norm_table, "tp")
    own_totals = lax.dynamic_slice_in_dim(totals, leading_head, head_count, 1)
    mean_sq = own_totals[..., None] / DV
    own_gain = lax.dynamic_slice_in_dim(head_norm_gain, value_start, head_width, 0)
    gate_part = jax.nn.silu(
        gate_rows.astype(jnp.float32).reshape(seq_count, head_count, head_width)
    )
    gated_rows = (
        (readout * lax.rsqrt(mean_sq + epsilon) * own_gain * gate_part)
        .reshape(seq_count, value_local)
        .astype(jnp.bfloat16)
    )
    partial_out = jnp.dot(gated_rows, output_matrix, preferred_element_type=jnp.float32)
    mixer_sum = lax.psum(partial_out.astype(jnp.bfloat16), "tp").astype(jnp.float32)
    blended_tokens = (stream.astype(jnp.float32) + mixer_sum).astype(jnp.bfloat16)
    normed_two = rms_scaled(blended_tokens, mixture_norm_gain)
    ep_count = lax.axis_size("ep")
    local_experts = expert_gate_weight.shape[0]
    experts_all = ep_count * local_experts
    route_count = expert_index_table.shape[1]
    capacity = 2 * seq_count * route_count // experts_all
    slot_count = experts_all * capacity
    flat_ids = expert_index_table.reshape(seq_count * route_count)
    one_hot = (flat_ids[:, None] == jnp.arange(experts_all, dtype=jnp.int32)[None, :]).astype(
        jnp.int32
    )
    rank_in = jnp.sum(one_hot * (jnp.cumsum(one_hot, axis=0) - 1), axis=1)
    place_lookup = flat_ids * capacity + rank_in
    placing = (place_lookup[:, None] == jnp.arange(slot_count, dtype=jnp.int32)[None, :]).astype(
        jnp.float32
    )
    placing = placing.reshape(seq_count, route_count, slot_count)
    logit_exp = jnp.exp(expert_scores_within)
    weights = logit_exp / jnp.sum(logit_exp, axis=-1, keepdims=True) * group_probability[:, None]
    combine = jnp.einsum("sk,skc->sc", weights, placing, precision=lax.Precision.HIGHEST)
    dispatch = jnp.sum(placing, axis=1).astype(jnp.bfloat16)
    outgoing = jnp.einsum("sc,sd->cd", dispatch, normed_two, preferred_element_type=jnp.float32)
    outgoing = outgoing.astype(jnp.bfloat16).reshape(experts_all, capacity, model_width)
    width_local = expert_down_weight.shape[2]
    arrived = lax.all_to_all(outgoing, "ep", split_axis=0, concat_axis=0, tiled=True)
    held_slots = arrived.shape[1]
    grouped = arrived.reshape(ep_count, local_experts, held_slots, model_width)
    gate_pre = jnp.einsum(
        "sxcd,xfd->sxcf", grouped, expert_gate_weight, preferred_element_type=jnp.float32
    )
    up_pre = jnp.einsum(
        "sxcd,xfd->sxcf", grouped, expert_up_weight, preferred_element_type=jnp.float32
    )
    hidden = (jax.nn.silu(gate_pre) * up_pre).astype(jnp.bfloat16)
    outputs = jnp.einsum(
        "sxcf,xfd->sxcd",
        lax.all_gather(hidden, "tp", axis=3, tiled=True),
        expert_down_weight,
        preferred_element_type=jnp.float32,
    )
    ready_rows = outputs.astype(jnp.bfloat16).reshape(
        ep_count * local_experts, held_slots, width_local
    )
    returned = lax.all_to_all(ready_rows, "ep", split_axis=0, concat_axis=0, tiled=True)
    mixture = jnp.dot(
        combine,
        returned.reshape(slot_count, width_local).astype(jnp.float32),
        precision=lax.Precision.HIGHEST,
    )
    own_mixed = lax.dynamic_slice_in_dim(blended_tokens, tp_index * width_local, width_local, 1)
    new_stream = (own_mixed.astype(jnp.float32) + mixture).astype(jnp.bfloat16)
    return (new_stream, updated.reshape(seq_count, KEY_CHANNELS, value_local))


def greet(partners):
    barrier = pltpu.get_barrier_semaphore()
    for partner in partners:
        pl.semaphore_signal(barrier, inc=1, device_id=partner, device_id_type=MESH)
    pl.semaphore_wait(barrier, len(partners))


def send(source, target, send_sem, recv_sem, partner):
    copy = pltpu.make_async_remote_copy(
        src_ref=source,
        dst_ref=target,
        send_sem=send_sem,
        recv_sem=recv_sem,
        device_id=partner,
        device_id_type=MESH,
    )
    copy.start()
    return copy


def project_kernel(
    n,
    stream_hbm,
    gain_hbm,
    query_hbm,
    key_hbm,
    value_hbm,
    gate_hbm,
    lower_hbm,
    upper_hbm,
    boost_hbm,
    state_hbm,
    output_hbm,
    expert_gate_hbm,
    expert_up_hbm,
    expert_down_hbm,
    fkq_ref,
    value_ref,
    gate_ref,
    state_ref,
    output_ref,
    expert_gate_ref,
    expert_up_ref,
    expert_down_ref,
    stream,
    gain,
    weights,
    lower,
    upper,
    boost,
    chunks,
    spread,
    near_out,
    near_in,
    mid_out,
    mid_in,
    far_out,
    far_in,
    held,
    load_sem,
    push_send,
    push_recv,
    chunk_send,
    chunk_recv,
    near_send,
    near_recv,
    mid_send,
    mid_recv,
    far_send,
    far_recv,
):
    me = lax.axis_index("ep")
    tp = lax.axis_index("tp")
    core = lax.rem(me, 2)
    row = me // 2
    rows = n // 2
    seqs = stream.shape[0]
    feats = query_hbm.shape[0]
    span = boost.shape[1]
    width = value_hbm.shape[1]
    columns = pl.ds(pl.multiple_of(tp * span, 128), span)
    mine = pl.ds(pl.multiple_of(core * feats, 128), feats)
    sources = [query_hbm.at[:, columns], key_hbm.at[:, columns], value_hbm, gate_hbm]
    places = [
        weights.at[mine, pl.ds(0, span)],
        weights.at[mine, pl.ds(span, span)],
        weights.at[mine, pl.ds(2 * span, width)],
        weights.at[mine, pl.ds(2 * span + width, width)],
    ]
    loads = [
        pltpu.make_async_copy(source, place, load_sem.at[i])
        for i, (source, place) in enumerate(zip(sources, places))
    ]
    small = [
        pltpu.make_async_copy(lower_hbm, lower, load_sem.at[4]),
        pltpu.make_async_copy(upper_hbm.at[:, columns], upper, load_sem.at[5]),
        pltpu.make_async_copy(boost_hbm.at[:, columns], boost, load_sem.at[6]),
    ]
    first = [
        pltpu.make_async_copy(stream_hbm, stream, load_sem.at[7]),
        pltpu.make_async_copy(gain_hbm, gain, load_sem.at[8]),
    ]
    later = [
        pltpu.make_async_copy(source, place, load_sem.at[9 + i])
        for i, (source, place) in enumerate(
            [
                (state_hbm, state_ref),
                (output_hbm, output_ref),
                (expert_gate_hbm, expert_gate_ref),
                (expert_up_hbm, expert_up_ref),
                (expert_down_hbm, expert_down_ref),
            ]
        )
    ]
    partner = {"ep": me + 1 - 2 * core}
    peers = [{"ep": lax.rem(me + 2 * d, n)} for d in range(1, rows)]
    barrier = pltpu.get_barrier_semaphore()
    for peer in [partner] + peers:
        pl.semaphore_signal(barrier, inc=1, device_id=peer, device_id_type=MESH)
    for load in first + small + loads:
        load.start()
    for load in first:
        load.wait()
    floats = stream[...].astype(F32)
    scale = lax.rsqrt(jnp.mean(floats * floats, axis=-1, keepdims=True) + epsilon)
    normed = (floats * scale * gain[...]).astype(BF16)
    for d in range(rows):
        chunks[d] = normed[:, d * 2 * feats : (d + 1) * 2 * feats]
    spread[row] = chunks[row]
    pl.semaphore_wait(barrier, rows)
    side = row // 2
    outer = (row == 0) | (row == 3)
    near = row + 1 - 2 * lax.rem(row, 2)
    inner_there = 2 - side
    outer_there = 3 - 3 * side
    order = [near, inner_there, outer_there]
    inside = lax.rem(row, 2) != side
    sent = []
    back = [near, 3 - near, 3 - row]
    for j, there in enumerate(back):
        sent.append(
            send(
                chunks.at[there],
                spread.at[row],
                chunk_send.at[j],
                chunk_recv.at[row],
                {"ep": there * 2 + core},
            )
        )
    pushes = [
        send(source, place, push_send.at[i], push_recv.at[i], partner)
        for i, (source, place) in enumerate(zip(sources, places))
    ]
    for load in later:
        load.start()
    for load in small:
        load.wait()
    nt = (((1,), (1,)), ((), ()))
    low_rank = lax.dot_general(normed, lower[...], nt, preferred_element_type=F32).astype(BF16)
    logit = jnp.dot(low_rank, upper[...], preferred_element_type=F32)
    log_sig = jnp.minimum(logit, 0.0) - jnp.log1p(jnp.exp(-jnp.abs(logit)))
    factor = jnp.exp(log_sig / forgetting_softness - boost[...])
    high = factor.astype(BF16).astype(F32)
    middle = (factor - high).astype(BF16).astype(F32)
    low = factor - high - middle
    steps = seqs // STEP
    for i in range(steps):
        cut = slice(i * STEP, (i + 1) * STEP)
        fkq_ref[i, 0:STEP] = high[cut]
        fkq_ref[i, STEP : 2 * STEP] = middle[cut]
        fkq_ref[i, 2 * STEP : 3 * STEP] = low[cut]
        fkq_ref[i, 5 * STEP : 6 * STEP] = jnp.zeros_like(low[cut])
    cuts = [(0, 2 * span), (2 * span, width), (2 * span + width, width)]
    needs = [(0, 1), (2,), (3,)]
    copies = list(sent) + list(pushes)

    def cut_of(ref, b, *lead):
        return ref.at[(*lead, slice(None), pl.ds(*cuts[b]))]

    def ready(b):
        for i in needs[b]:
            loads[i].wait()
            pushes[i].wait_recv()

    def part_of(source, b):
        start, size = cuts[b]
        return jnp.dot(
            spread[source], weights[:, start : start + size], preferred_element_type=F32
        )

    def arrival(there):
        return pltpu.make_async_remote_copy(
            src_ref=chunks.at[0],
            dst_ref=spread.at[there],
            send_sem=chunk_send.at[0],
            recv_sem=chunk_recv.at[there],
            device_id=partner,
            device_id_type=MESH,
        )

    arrival(near).wait_recv()
    for b in range(3):
        ready(b)
        start, size = cuts[b]
        near_out[:, start : start + size] = part_of(near, b).astype(BF16)
        copies.append(
            send(
                cut_of(near_out, b),
                cut_of(near_in, b),
                near_send.at[b],
                near_recv.at[b],
                {"ep": near * 2 + core},
            )
        )
    arrival(inner_there).wait_recv()
    for b in range(3):
        start, size = cuts[b]
        part = part_of(inner_there, b)
        held[:, start : start + size] = part
        mid_out[:, start : start + size] = part.astype(BF16)

        @pl.when(jnp.logical_not(inside))
        def _():
            send(
                cut_of(mid_out, b),
                cut_of(mid_in, b),
                mid_send.at[b],
                mid_recv.at[b],
                {"ep": near * 2 + core},
            )

    arrival(outer_there).wait_recv()
    slot = jnp.where(inside, 0, 1)
    for b in range(3):
        start, size = cuts[b]
        far_out[:, start : start + size] = part_of(outer_there, b).astype(BF16)
        copies.append(
            send(
                cut_of(far_out, b),
                cut_of(far_in, b, slot),
                far_send.at[b],
                far_recv.at[slot, b],
                {"ep": outer_there * 2 + core},
            )
        )

    def middle_copy(b):
        return pltpu.make_async_remote_copy(
            src_ref=cut_of(mid_out, b),
            dst_ref=cut_of(far_in, b, 0),
            send_sem=mid_send.at[b],
            recv_sem=far_recv.at[0, b],
            device_id={"ep": inner_there * 2 + core},
            device_id_type=MESH,
        )

    def waiting(target, b, sem):
        return pltpu.make_async_remote_copy(
            src_ref=cut_of(mid_out, b),
            dst_ref=target,
            send_sem=mid_send.at[b],
            recv_sem=sem,
            device_id=partner,
            device_id_type=MESH,
        )

    @pl.when(inside)
    def _():
        for b in range(3):
            start, size = cuts[b]
            waiting(cut_of(mid_in, b), b, mid_recv.at[b]).wait_recv()
            merged = held[:, start : start + size] + mid_in[:, start : start + size].astype(F32)
            mid_out[:, start : start + size] = merged.astype(BF16)
            middle_copy(b).start()

    for b in range(3):
        start, size = cuts[b]
        held[:, start : start + size] = part_of(row, b)
    for b in range(3):
        start, size = cuts[b]
        waiting(cut_of(near_in, b), b, near_recv.at[b]).wait_recv()
        waiting(cut_of(far_in, b, 0), b, far_recv.at[0, b]).wait_recv()
        held[:, start : start + size] += near_in[:, start : start + size].astype(F32) + far_in[
            0, :, start : start + size
        ].astype(F32)

        @pl.when(jnp.logical_not(inside))
        def _():
            waiting(cut_of(far_in, b, 1), b, far_recv.at[1, b]).wait_recv()
            held[:, start : start + size] += far_in[1, :, start : start + size].astype(F32)

        total = held[:, start : start + size]
        if b == 0:
            query = (total[:, :span] * KEY_CHANNELS ** (-0.5)).astype(BF16).astype(F32)
            key = total[:, span:].astype(BF16).astype(F32)
            for i in range(steps):
                cut = slice(i * STEP, (i + 1) * STEP)
                fkq_ref[i, 3 * STEP : 4 * STEP] = key[cut]
                fkq_ref[i, 4 * STEP : 5 * STEP] = query[cut]
        else:
            target = value_ref if b == 1 else gate_ref
            total = total.astype(BF16).astype(F32)
            for i in range(steps):
                target[i] = total[i * STEP : (i + 1) * STEP]
    for copy in copies:
        copy.wait_send()
    for b in range(3):
        middle_copy(b).wait_send()
    for load in later:
        load.wait()


def state_kernel(state_ref, fkq_ref, value_ref, new_hbm, read_ref, spots, wide, buffer, out_sem):
    seqs, _, width = state_ref.shape
    heads = width // DV
    steps = seqs // STEP
    lines = fkq_ref.shape[1]
    line = lax.broadcasted_iota(jnp.int32, (lines, 3 * STEP * KEY_CHANNELS), 0)
    block = lax.broadcasted_iota(jnp.int32, (lines, 3 * STEP * KEY_CHANNELS), 1) // KEY_CHANNELS
    kind = jnp.maximum(line // STEP - 2, 0)
    wanted = (block // STEP == kind) & (block % STEP == line % STEP) & (line < 5 * STEP)
    spots[...] = wanted.astype(F32).astype(BF16)

    def flush(s):
        return pltpu.make_async_copy(buffer.at[s], new_hbm.at[s], out_sem.at[s])

    @pl.loop(0, steps)
    def _(i):
        for h in range(heads):
            turned = fkq_ref[i, :, h * KEY_CHANNELS : (h + 1) * KEY_CHANNELS].T.astype(BF16)
            wide[h] = jnp.dot(turned, spots[...], preferred_element_type=F32)
        for s in range(STEP):
            sums = []
            for h in range(heads):
                factor, key, query = (
                    wide[h, :, (j * STEP + s) * KEY_CHANNELS : (j * STEP + s + 1) * KEY_CHANNELS]
                    for j in range(3)
                )
                for g in range(DV // KEY_CHANNELS):
                    start = h * DV + g * KEY_CHANNELS
                    lanes = slice(start, start + KEY_CHANNELS)
                    updated = factor * state_ref[i * STEP + s, :, lanes] + key * value_ref[
                        i, s : s + 1, lanes
                    ]
                    buffer[i * STEP + s, :, lanes] = updated
                    sums.append(jnp.sum((query * updated).reshape(-1, 8, KEY_CHANNELS), axis=0))
            read_ref[i * STEP + s] = jnp.concatenate(sums, axis=1)
            flush(i * STEP + s).start()

    for s in range(seqs):
        flush(s).wait()


def mixture_kernel(
    n,
    m,
    read_ref,
    rows_ref,
    head_gain_ref,
    stream_hbm,
    gain_ref,
    index_ref,
    score_ref,
    prob_ref,
    w_out,
    w_gate,
    w_up,
    w_down,
    out_ref,
    own_stream,
    lhs,
    part_out,
    part_in,
    slots_out,
    shares_out,
    shares_in,
    arrived,
    hidden_out,
    hidden_in,
    pair_down,
    ready,
    returned,
    load_sem,
    part_send,
    part_recv,
    slot_send,
    slot_recv,
    share_send,
    share_recv,
    join_send,
    join_recv,
    swap_send,
    swap_recv,
    push_send,
    push_recv,
    hid_send,
    hid_recv,
    back_send,
    back_recv,
):
    me = lax.axis_index("ep")
    tp = lax.axis_index("tp")
    core = lax.rem(me, 2)
    row = me // 2
    rows = n // 2
    seqs, width = own_stream.shape
    capacity = slots_out.shape[1]
    half = rows * capacity
    inner = w_gate.shape[1]
    tps = [m - 1 - tp, tp + 1 - 2 * lax.rem(tp, 2), lax.rem(tp + 2, m)]
    near = row + 1 - 2 * lax.rem(row, 2)
    zs = [3 - row, 3 - near, near]
    other = me + 1 - 2 * core
    partners = (
        [{"tp": t} for t in tps]
        + [{"ep": z * 2 + core} for z in zs]
        + [{"ep": other}]
        + [{"tp": t, "ep": other} for t in tps]
    )
    barrier = pltpu.get_barrier_semaphore()
    for partner in partners:
        pl.semaphore_signal(barrier, inc=1, device_id=partner, device_id_type=MESH)
    own_cut = pl.ds(pl.multiple_of(tp * width, 128), width)
    load = pltpu.make_async_copy(stream_hbm.at[:, own_cut], own_stream, load_sem.at[0])
    load.start()
    for i in range(seqs // STEP):
        lhs[i * STEP : (i + 1) * STEP] = rows_ref[i]
    gates = lhs[...]
    silu = gates / (1.0 + jnp.exp(-gates))
    readout = jnp.sum(read_ref[...], axis=1)
    for h in range(width // DV):
        lanes = slice(h * DV, (h + 1) * DV)
        part = readout[:, lanes]
        mean_sq = jnp.mean(part * part, axis=-1, keepdims=True)
        lhs[:, lanes] = part * lax.rsqrt(mean_sq + epsilon) * head_gain_ref[...] * silu[:, lanes]
    gated = lhs[...].astype(BF16)
    done = []
    parts = []
    for j, there in enumerate(tps + [tp]):
        cut = pl.ds(pl.multiple_of(there * width, 128), width)
        part = jnp.dot(gated, w_out[:, cut], preferred_element_type=F32)
        if j == 0:
            pl.semaphore_wait(barrier, len(partners))
        if j < m - 1:
            part_out[j] = part.astype(BF16)
            parts.append(
                send(part_out.at[j], part_in.at[j], part_send.at[j], part_recv.at[j], {"tp": there})
            )
    push = send(w_down.at[0], pair_down, push_send.at[0], push_recv.at[0], {"ep": other})

    index = index_ref[...]
    group = index[0:1] // 2
    band = lax.broadcasted_iota(jnp.int32, (8, seqs), 0)
    one_hot = (band == group).astype(F32)
    earlier = lax.broadcasted_iota(jnp.int32, (seqs, seqs), 0) < lax.broadcasted_iota(
        jnp.int32, (seqs, seqs), 1
    )
    counts = jnp.dot(one_hot, earlier.astype(F32), preferred_element_type=F32)
    rank = jnp.sum(counts * one_hot, axis=0, keepdims=True).astype(jnp.int32)
    slot_line = lax.broadcasted_iota(jnp.int32, (GROUPS * capacity, seqs), 0)
    placing = (slot_line == group * capacity + rank).astype(F32)
    scores = jnp.exp(score_ref[...])
    shares = scores / jnp.sum(scores, axis=0, keepdims=True) * prob_ref[...]
    place_line = lax.broadcasted_iota(jnp.int32, (128, seqs), 0)
    table = jnp.zeros((128, seqs), F32)
    for k in range(index.shape[0]):
        table += jnp.where(place_line == lax.rem(index[k : k + 1], 2), shares[k : k + 1], 0.0)
    nt = (((1,), (1,)), ((), ()))
    shares_out[...] = lax.dot_general(
        placing, table, nt, preferred_element_type=F32, precision=lax.Precision.HIGHEST
    ).reshape(GROUPS, capacity, 128)
    placing = placing.astype(BF16)

    for z in zs:
        done.append(
            send(
                shares_out.at[z],
                shares_in.at[row],
                share_send.at[z],
                share_recv.at[row],
                {"ep": z * 2 + core},
            )
        )
    shares_in[row] = shares_out[row]
    load.wait()
    total = part + own_stream[...].astype(F32)
    for j in (1, 2, 0):
        parts[j].wait_recv()
        total = total + part_in[j].astype(F32)
    mixed = total.astype(BF16)
    slots = jnp.dot(placing, mixed, preferred_element_type=F32)
    slots_out[...] = slots.reshape(GROUPS, capacity, width).astype(BF16)
    for z in zs:
        done.append(
            send(
                slots_out.at[z],
                arrived.at[tp, core, row],
                slot_send.at[z],
                slot_recv.at[row],
                {"ep": z * 2 + core},
            )
        )
    arrived[tp, core, row] = slots_out[row]

    def swap(t, z):
        done.append(
            send(
                arrived.at[t, core, z],
                arrived.at[t, core, z],
                swap_send.at[t, z],
                swap_recv.at[t, z],
                {"ep": other},
            )
        )

    def join(z):
        for t in tps:
            done.append(
                send(
                    arrived.at[tp, core, z],
                    arrived.at[tp, core, z],
                    join_send.at[t, z],
                    join_recv.at[tp, z],
                    {"tp": t},
                )
            )
        swap(tp, z)

    def expect(target, sem):
        pltpu.make_async_remote_copy(
            src_ref=target,
            dst_ref=target,
            send_sem=sem,
            recv_sem=sem,
            device_id={"ep": other},
            device_id_type=MESH,
        ).wait_recv()

    def relay(z):
        for t in (tps[1], tps[2], tps[0]):
            expect(arrived.at[t, core, z], join_recv.at[t, z])
            swap(t, z)

    order = [row] + zs[::-1]
    join(row)
    expect(arrived.at[tp, core, order[1]], slot_recv.at[order[1]])
    join(order[1])
    expect(arrived.at[tp, core, order[2]], slot_recv.at[order[2]])
    join(order[2])
    relay(order[0])
    expect(arrived.at[tp, core, order[3]], slot_recv.at[order[3]])
    join(order[3])
    relay(order[1])
    relay(order[2])

    tokens_held = n * capacity
    square = jnp.zeros((tokens_held, 1), F32)
    gate_pre = jnp.zeros((tokens_held, inner), F32)
    up_pre = jnp.zeros((tokens_held, inner), F32)
    for j, t in enumerate([tp, tps[1], tps[2], tps[0]]):
        if j == 1:
            relay(order[3])
        for z in order:
            expect(arrived.at[t, 1 - core, z], swap_recv.at[t, z])
        cut = pl.ds(pl.multiple_of(t * width, 128), width)
        tokens = arrived[t].astype(F32).reshape(tokens_held, width)
        square += jnp.sum(tokens * tokens, axis=-1, keepdims=True)
        scaled = (tokens * gain_ref[:, cut]).astype(BF16)
        gate_pre += lax.dot_general(scaled, w_gate[0, :, cut], nt, preferred_element_type=F32)
        up_pre += lax.dot_general(scaled, w_up[0, :, cut], nt, preferred_element_type=F32)
    scale = lax.rsqrt(square / (m * width) + epsilon)
    gate_pre *= scale
    up_pre *= scale
    hidden_out[...] = (
        (gate_pre / (1.0 + jnp.exp(-gate_pre)) * up_pre).astype(BF16).reshape(2, half, inner)
    )
    for j, t in enumerate(tps):
        for c in range(2):
            done.append(
                send(
                    hidden_out.at[c],
                    hidden_in.at[core, tp],
                    hid_send.at[2 * j + c],
                    hid_recv.at[core, tp],
                    {"tp": t, "ep": row * 2 + c},
                )
            )
    done.append(
        send(
            hidden_out.at[1 - core],
            hidden_in.at[core, tp],
            hid_send.at[2 * m - 2],
            hid_recv.at[core, tp],
            {"ep": other},
        )
    )
    hidden_in[core, tp] = hidden_out[core]
    push.wait_recv()
    own_sum = jnp.zeros((half, width), F32)
    pair_sum = jnp.zeros((half, width), F32)
    for j, t in enumerate([tp, tps[1], tps[2], tps[0]]):
        lines = pl.ds(pl.multiple_of(t * inner, 128), inner)
        if j > 0:
            expect(hidden_in.at[core, t], hid_recv.at[core, t])
        own_sum += jnp.dot(hidden_in[core, t], w_down[0, lines, :], preferred_element_type=F32)
        expect(hidden_in.at[1 - core, t], hid_recv.at[1 - core, t])
        pair_sum += jnp.dot(hidden_in[1 - core, t], pair_down[lines, :], preferred_element_type=F32)
    for z in zs:
        expect(shares_in.at[z], share_recv.at[z])
    share = shares_in[...].reshape(half, 128)
    which = lax.broadcasted_iota(jnp.int32, (half, 128), 1)
    own_share = jnp.sum(jnp.where(which == core, share, 0.0), axis=1, keepdims=True)
    pair_share = jnp.sum(jnp.where(which == 1 - core, share, 0.0), axis=1, keepdims=True)
    outputs = own_share * own_sum.astype(BF16).astype(F32) + pair_share * pair_sum.astype(
        BF16
    ).astype(F32)
    ready[...] = outputs.reshape(rows, capacity, width).astype(BF16)
    for z in zs:
        done.append(
            send(
                ready.at[z],
                returned.at[row],
                back_send.at[z],
                back_recv.at[row],
                {"ep": z * 2 + core},
            )
        )
    returned[row] = ready[row]
    for z in zs[::-1]:
        expect(returned.at[z], back_recv.at[z])
    mixture = lax.dot_general(
        placing,
        returned[...].reshape(half, width),
        (((0,), (0,)), ((), ())),
        preferred_element_type=F32,
    )
    out_ref[...] = (mixed.astype(F32) + mixture).astype(BF16)
    for copy in parts + done + [push]:
        copy.wait_send()


def fused(
    stream,
    previous_state,
    mixer_norm_gain,
    query_matrix,
    key_matrix,
    value_matrix,
    output_gate_weight,
    decay_lower_factor,
    decay_upper_factor,
    forgetting_boost,
    head_norm_gain,
    output_matrix,
    mixture_norm_gain,
    expert_gate_weight,
    expert_up_weight,
    expert_down_weight,
    expert_index_table,
    expert_scores_within,
    group_probability,
):
    n = lax.axis_size("ep")
    m = lax.axis_size("tp")
    seqs, model = stream.shape
    width = previous_state.shape[2]
    span = width // DV * KEY_CHANNELS
    feats = query_matrix.shape[0]
    rank = decay_lower_factor.shape[1]
    steps = seqs // STEP
    total = 2 * span + 2 * width
    rows = n // 2
    dma = pltpu.SemaphoreType.DMA
    vmem = pl.BlockSpec(memory_space=pltpu.VMEM)
    hbm = pl.BlockSpec(memory_space=pltpu.HBM)
    ahead = (
        previous_state,
        output_matrix,
        expert_gate_weight,
        expert_up_weight,
        expert_down_weight,
    )
    fkq, values, gates, *held = pl.pallas_call(
        functools.partial(project_kernel, n),
        name="project",
        out_shape=(
            jax.ShapeDtypeStruct((steps, 6 * STEP, span), F32),
            jax.ShapeDtypeStruct((steps, STEP, width), F32),
            jax.ShapeDtypeStruct((steps, STEP, width), F32),
            *(pltpu.VMEM(a.shape, a.dtype) for a in ahead),
        ),
        in_specs=[hbm] * (9 + len(ahead)),
        out_specs=(vmem,) * (3 + len(ahead)),
        scratch_shapes=[
            pltpu.VMEM((seqs, model), BF16),
            pltpu.VMEM((1, model), F32),
            pltpu.VMEM((2 * feats, total), BF16),
            pltpu.VMEM((rank, model), BF16),
            pltpu.VMEM((rank, span), BF16),
            pltpu.VMEM((seqs, span), F32),
            pltpu.VMEM((rows, seqs, 2 * feats), BF16),
            pltpu.VMEM((rows, seqs, 2 * feats), BF16),
            pltpu.VMEM((seqs, total), BF16),
            pltpu.VMEM((seqs, total), BF16),
            pltpu.VMEM((seqs, total), BF16),
            pltpu.VMEM((seqs, total), BF16),
            pltpu.VMEM((seqs, total), BF16),
            pltpu.VMEM((2, seqs, total), BF16),
            pltpu.VMEM((seqs, total), F32),
            dma((14,)),
            dma((4,)),
            dma((4,)),
            dma((rows,)),
            dma((rows,)),
            dma((3,)),
            dma((3,)),
            dma((3,)),
            dma((3,)),
            dma((3,)),
            dma((2, 3)),
        ],
        compiler_params=pltpu.CompilerParams(
            collective_id=0, has_side_effects=True, vmem_limit_bytes=12 * 2**20
        ),
        cost_estimate=pl.CostEstimate(flops=COST, bytes_accessed=3 * feats * total, transcendentals=0),
    )(
        *(pltpu.with_memory_space_constraint(a, pltpu.HBM) for a in (
            stream,
            mixer_norm_gain.reshape(1, model),
            query_matrix,
            key_matrix,
            value_matrix,
            output_gate_weight,
            decay_lower_factor.T,
            decay_upper_factor,
            forgetting_boost,
            *ahead,
        ))
    )
    previous_state, output_matrix, expert_gate_weight, expert_up_weight, expert_down_weight = held
    new_state, readout = pl.pallas_call(
        state_kernel,
        name="state",
        out_shape=(
            jax.ShapeDtypeStruct(previous_state.shape, F32),
            jax.ShapeDtypeStruct((seqs, 8, width), F32),
        ),
        in_specs=[vmem, vmem, vmem],
        out_specs=(hbm, vmem),
        scratch_shapes=[
            pltpu.VMEM((6 * STEP, 3 * STEP * KEY_CHANNELS), BF16),
            pltpu.VMEM((width // DV, KEY_CHANNELS, 3 * STEP * KEY_CHANNELS), F32),
            pltpu.VMEM(previous_state.shape, F32),
            dma((seqs,)),
        ],
        compiler_params=pltpu.CompilerParams(vmem_limit_bytes=14 * 2**20),
        cost_estimate=pl.CostEstimate(
            flops=COST // 4, bytes_accessed=4 * previous_state.size, transcendentals=0
        ),
    )(previous_state, fkq, values)
    inner = expert_gate_weight.shape[1]
    capacity = 2 * seqs * expert_index_table.shape[1] // n
    new_stream = pl.pallas_call(
        functools.partial(mixture_kernel, n, m),
        name="mixture",
        out_shape=jax.ShapeDtypeStruct((seqs, width), BF16),
        in_specs=[vmem] * 3 + [hbm] + [vmem] * 8,
        out_specs=vmem,
        scratch_shapes=[
            pltpu.VMEM((seqs, width), BF16),
            pltpu.VMEM((seqs, width), F32),
            pltpu.VMEM((m - 1, seqs, width), BF16),
            pltpu.VMEM((m - 1, seqs, width), BF16),
            pltpu.VMEM((GROUPS, capacity, width), BF16),
            pltpu.VMEM((GROUPS, capacity, 128), F32),
            pltpu.VMEM((GROUPS, capacity, 128), F32),
            pltpu.VMEM((m, 2, rows, capacity, width), BF16),
            pltpu.VMEM((2, rows * capacity, inner), BF16),
            pltpu.VMEM((2, m, rows * capacity, inner), BF16),
            pltpu.VMEM(expert_down_weight.shape[1:], BF16),
            pltpu.VMEM((rows, capacity, width), BF16),
            pltpu.VMEM((rows, capacity, width), BF16),
            dma((1,)),
            dma((m - 1,)),
            dma((m - 1,)),
            dma((rows,)),
            dma((rows,)),
            dma((rows,)),
            dma((rows,)),
            dma((m, rows)),
            dma((m, rows)),
            dma((m, rows)),
            dma((m, rows)),
            dma((1,)),
            dma((1,)),
            dma((2 * m - 1,)),
            dma((2, m)),
            dma((rows,)),
            dma((rows,)),
        ],
        compiler_params=pltpu.CompilerParams(
            collective_id=1, has_side_effects=True, vmem_limit_bytes=VM3 * 2**20
        ),
        cost_estimate=pl.CostEstimate(flops=COST, bytes_accessed=2 * output_matrix.size, transcendentals=0),
    )(
        readout,
        gates,
        head_norm_gain.reshape(1, DV),
        stream,
        mixture_norm_gain.reshape(1, model),
        expert_index_table.T,
        expert_scores_within.T,
        group_probability.reshape(1, seqs),
        output_matrix,
        expert_gate_weight,
        expert_up_weight,
        expert_down_weight,
    )
    return (new_stream, new_state)


def on_device(*arrays):
    stream, state = arrays[0], arrays[1]
    experts_held, route_count = arrays[13].shape[0], arrays[16].shape[1]
    n = lax.axis_size("ep")
    whole_heads = state.shape[2] % DV == 0
    pair_routed = experts_held == 1 and n == GROUPS * route_count and route_count == 2
    boxed = n == 8 and lax.axis_size("tp") == 4
    full_tiles = stream.shape[0] % 16 == 0 and stream.shape[1] == state.shape[2] * lax.axis_size("tp")
    if whole_heads and pair_routed and full_tiles and boxed:
        return fused(*arrays)
    return general(*arrays)


def solution(mesh):
    placed = (
        P("ep", None),
        P("ep", None, "tp"),
        P(),
        P("ep", None),
        P("ep", None),
        P("ep", "tp"),
        P("ep", "tp"),
        P(),
        P(),
        P("ep", None),
        P(),
        P("tp", None),
        P(),
        P("ep", "tp", None),
        P("ep", "tp", None),
        P("ep", None, "tp"),
        P("ep", None),
        P("ep", None),
        P("ep"),
    )
    return jax.shard_map(
        on_device,
        mesh=mesh,
        in_specs=placed,
        out_specs=(P("ep", "tp"), P("ep", None, "tp")),
        check_vma=False,
    )
```

```python
import functools

import jax
import jax.numpy as jnp
from jax import lax
from jax.experimental import pallas as pl
from jax.experimental.pallas import tpu as pltpu
from jax.sharding import PartitionSpec as P

HEAD_TOTAL = 16
KEY_CHANNELS = 128
DV = 256
GROUPS = 4
STEP = 4
COST = 20_000_000_000
GRANT = 40
F32 = jnp.float32
BF16 = jnp.bfloat16
MESH = pl.DeviceIdType.MESH

epsilon = 1e-06
forgetting_softness = 16.0


def rms_scaled(values, gain_vec):
    floats = values.astype(jnp.float32)
    scaled = floats * lax.rsqrt(jnp.mean(floats * floats, axis=-1, keepdims=True) + epsilon)
    return (scaled * gain_vec).astype(jnp.bfloat16)


def general(
    stream,
    previous_state,
    mixer_norm_gain,
    query_matrix,
    key_matrix,
    value_matrix,
    output_gate_weight,
    decay_lower_factor,
    decay_upper_factor,
    forgetting_boost,
    head_norm_gain,
    output_matrix,
    mixture_norm_gain,
    expert_gate_weight,
    expert_up_weight,
    expert_down_weight,
    expert_index_table,
    expert_scores_within,
    group_probability,
):
    seq_count, model_width = stream.shape
    value_local = previous_state.shape[2]
    head_count = max(1, value_local // DV)
    head_width = min(value_local, DV)
    tp_index = lax.axis_index("tp")
    leading_head = tp_index * value_local // DV
    value_start = tp_index * value_local % DV
    key_column_span = head_count * KEY_CHANNELS
    normed = rms_scaled(stream, mixer_norm_gain)
    own_query = lax.dynamic_slice_in_dim(
        query_matrix, leading_head * KEY_CHANNELS, key_column_span, 1
    )
    own_key = lax.dynamic_slice_in_dim(key_matrix, leading_head * KEY_CHANNELS, key_column_span, 1)
    spread = lax.all_to_all(normed, "ep", split_axis=1, concat_axis=0, tiled=True)
    joined = jnp.concatenate([own_query, own_key, value_matrix, output_gate_weight], axis=1)
    summed = lax.psum_scatter(
        jnp.dot(spread, joined, preferred_element_type=jnp.float32),
        "ep",
        scatter_dimension=0,
        tiled=True,
    )
    query_sum = summed[:, :key_column_span]
    key_sum = summed[:, key_column_span : 2 * key_column_span]
    value_sum = summed[:, 2 * key_column_span : 2 * key_column_span + value_local]
    gate_sum = summed[:, 2 * key_column_span + value_local :]
    queries = (query_sum * KEY_CHANNELS ** (-0.5)).astype(jnp.bfloat16)
    key_rows = key_sum.astype(jnp.bfloat16)
    value_rows = value_sum.astype(jnp.bfloat16)
    gate_rows = gate_sum.astype(jnp.bfloat16)
    low_rank = jnp.dot(normed, decay_lower_factor, preferred_element_type=jnp.float32).astype(
        jnp.bfloat16
    )
    local_expand_matrix = lax.dynamic_slice_in_dim(
        decay_upper_factor, leading_head * KEY_CHANNELS, key_column_span, 1
    )
    forgetting_logit = jnp.dot(low_rank, local_expand_matrix, preferred_element_type=jnp.float32)
    request_boost = lax.dynamic_slice_in_dim(
        forgetting_boost, leading_head * KEY_CHANNELS, key_column_span, 1
    )
    forgetting_lograte = jax.nn.log_sigmoid(forgetting_logit) / forgetting_softness - request_boost
    factor = (
        jnp.exp(forgetting_lograte)
        .reshape(seq_count, head_count, KEY_CHANNELS)
        .transpose(0, 2, 1)[..., None]
    )
    state_four = previous_state.reshape(seq_count, KEY_CHANNELS, head_count, head_width)
    key_part = (
        key_rows.astype(jnp.float32)
        .reshape(seq_count, head_count, KEY_CHANNELS)
        .transpose(0, 2, 1)[..., None]
    )
    value_part = value_rows.astype(jnp.float32).reshape(seq_count, 1, head_count, head_width)
    updated = factor * state_four + key_part * value_part
    query_part = (
        queries.astype(jnp.float32).reshape(seq_count, head_count, KEY_CHANNELS).transpose(0, 2, 1)
    )
    readout = jnp.einsum("skh,skhv->shv", query_part, updated, precision=lax.Precision.HIGHEST)
    square_sums = jnp.sum(readout * readout, axis=-1)
    norm_table = lax.dynamic_update_slice(
        jnp.zeros((seq_count, HEAD_TOTAL), jnp.float32), square_sums, (jnp.int32(0), leading_head)
    )
    totals = lax.psum(norm_table, "tp")
    own_totals = lax.dynamic_slice_in_dim(totals, leading_head, head_count, 1)
    mean_sq = own_totals[..., None] / DV
    own_gain = lax.dynamic_slice_in_dim(head_norm_gain, value_start, head_width, 0)
    gate_part = jax.nn.silu(
        gate_rows.astype(jnp.float32).reshape(seq_count, head_count, head_width)
    )
    gated_rows = (
        (readout * lax.rsqrt(mean_sq + epsilon) * own_gain * gate_part)
        .reshape(seq_count, value_local)
        .astype(jnp.bfloat16)
    )
    partial_out = jnp.dot(gated_rows, output_matrix, preferred_element_type=jnp.float32)
    mixer_sum = lax.psum(partial_out.astype(jnp.bfloat16), "tp").astype(jnp.float32)
    blended_tokens = (stream.astype(jnp.float32) + mixer_sum).astype(jnp.bfloat16)
    normed_two = rms_scaled(blended_tokens, mixture_norm_gain)
    ep_count = lax.axis_size("ep")
    local_experts = expert_gate_weight.shape[0]
    experts_all = ep_count * local_experts
    route_count = expert_index_table.shape[1]
    capacity = 2 * seq_count * route_count // experts_all
    slot_count = experts_all * capacity
    flat_ids = expert_index_table.reshape(seq_count * route_count)
    one_hot = (flat_ids[:, None] == jnp.arange(experts_all, dtype=jnp.int32)[None, :]).astype(
        jnp.int32
    )
    rank_in = jnp.sum(one_hot * (jnp.cumsum(one_hot, axis=0) - 1), axis=1)
    place_lookup = flat_ids * capacity + rank_in
    placing = (place_lookup[:, None] == jnp.arange(slot_count, dtype=jnp.int32)[None, :]).astype(
        jnp.float32
    )
    placing = placing.reshape(seq_count, route_count, slot_count)
    logit_exp = jnp.exp(expert_scores_within)
    weights = logit_exp / jnp.sum(logit_exp, axis=-1, keepdims=True) * group_probability[:, None]
    combine = jnp.einsum("sk,skc->sc", weights, placing, precision=lax.Precision.HIGHEST)
    dispatch = jnp.sum(placing, axis=1).astype(jnp.bfloat16)
    outgoing = jnp.einsum("sc,sd->cd", dispatch, normed_two, preferred_element_type=jnp.float32)
    outgoing = outgoing.astype(jnp.bfloat16).reshape(experts_all, capacity, model_width)
    width_local = expert_down_weight.shape[2]
    arrived = lax.all_to_all(outgoing, "ep", split_axis=0, concat_axis=0, tiled=True)
    held_slots = arrived.shape[1]
    grouped = arrived.reshape(ep_count, local_experts, held_slots, model_width)
    gate_pre = jnp.einsum(
        "sxcd,xfd->sxcf", grouped, expert_gate_weight, preferred_element_type=jnp.float32
    )
    up_pre = jnp.einsum(
        "sxcd,xfd->sxcf", grouped, expert_up_weight, preferred_element_type=jnp.float32
    )
    hidden = (jax.nn.silu(gate_pre) * up_pre).astype(jnp.bfloat16)
    outputs = jnp.einsum(
        "sxcf,xfd->sxcd",
        lax.all_gather(hidden, "tp", axis=3, tiled=True),
        expert_down_weight,
        preferred_element_type=jnp.float32,
    )
    ready_rows = outputs.astype(jnp.bfloat16).reshape(
        ep_count * local_experts, held_slots, width_local
    )
    returned = lax.all_to_all(ready_rows, "ep", split_axis=0, concat_axis=0, tiled=True)
    mixture = jnp.dot(
        combine,
        returned.reshape(slot_count, width_local).astype(jnp.float32),
        precision=lax.Precision.HIGHEST,
    )
    own_mixed = lax.dynamic_slice_in_dim(blended_tokens, tp_index * width_local, width_local, 1)
    new_stream = (own_mixed.astype(jnp.float32) + mixture).astype(jnp.bfloat16)
    return (new_stream, updated.reshape(seq_count, KEY_CHANNELS, value_local))


def send(source, target, send_sem, recv_sem, partner):
    copy = pltpu.make_async_remote_copy(
        src_ref=source,
        dst_ref=target,
        send_sem=send_sem,
        recv_sem=recv_sem,
        device_id=partner,
        device_id_type=MESH,
    )
    copy.start()
    return copy


def layer_kernel(
    n,
    m,
    stream_hbm,
    gain_hbm,
    query_hbm,
    key_hbm,
    value_hbm,
    gate_hbm,
    lower_hbm,
    upper_hbm,
    boost_hbm,
    head_gain_hbm,
    gain_two_hbm,
    index_hbm,
    score_hbm,
    prob_hbm,
    state_hbm,
    output_hbm,
    expert_gate_hbm,
    expert_up_hbm,
    expert_down_hbm,
    state_ref,
    out_ref,
    stream,
    gain,
    weights,
    lower,
    upper,
    boost,
    head_gain_ref,
    gain_ref,
    index_ref,
    score_ref,
    prob_ref,
    w_out,
    w_gate,
    w_up,
    w_down,
    pair_down,
    chunks,
    spread,
    near_out,
    near_in,
    mid_out,
    mid_in,
    far_out,
    far_in,
    held,
    lines,
    turned,
    spots,
    wide,
    values,
    read,
    part_out,
    part_in,
    slots_out,
    shares_out,
    shares_in,
    arrived,
    hidden_out,
    hidden_in,
    ready,
    returned,
    load_sem,
    push_send,
    push_recv,
    chunk_send,
    chunk_recv,
    near_send,
    near_recv,
    mid_send,
    mid_recv,
    far_send,
    far_recv,
    part_send,
    part_recv,
    slot_send,
    slot_recv,
    share_send,
    share_recv,
    join_send,
    join_recv,
    swap_send,
    swap_recv,
    hid_send,
    hid_recv,
    back_send,
    back_recv,
):
    me = lax.axis_index("ep")
    tp = lax.axis_index("tp")
    core = lax.rem(me, 2)
    row = me // 2
    rows = n // 2
    seqs = stream.shape[0]
    feats = query_hbm.shape[0]
    span = boost.shape[1]
    width = value_hbm.shape[1]
    heads = width // DV
    steps = seqs // STEP
    capacity = slots_out.shape[1]
    half = rows * capacity
    inner = w_gate.shape[1]
    nt = (((1,), (1,)), ((), ()))
    side = row // 2
    inside = lax.rem(row, 2) != side
    near = row + 1 - 2 * lax.rem(row, 2)
    inner_there = 2 - side
    outer_there = 3 - 3 * side
    other = me + 1 - 2 * core
    partner = {"ep": other}
    zs = [3 - row, 3 - near, near]
    tps = [m - 1 - tp, tp + 1 - 2 * lax.rem(tp, 2), lax.rem(tp + 2, m)]
    partners = (
        [partner]
        + [{"ep": z * 2 + core} for z in zs]
        + [{"tp": t} for t in tps]
        + [{"tp": t, "ep": other} for t in tps]
    )
    barrier = pltpu.get_barrier_semaphore()
    for there in partners:
        pl.semaphore_signal(barrier, inc=1, device_id=there, device_id_type=MESH)

    columns = pl.ds(pl.multiple_of(tp * span, 128), span)
    mine = pl.ds(pl.multiple_of(core * feats, 128), feats)
    sources = [query_hbm.at[:, columns], key_hbm.at[:, columns], value_hbm, gate_hbm]
    places = [
        weights.at[mine, pl.ds(0, span)],
        weights.at[mine, pl.ds(span, span)],
        weights.at[mine, pl.ds(2 * span, width)],
        weights.at[mine, pl.ds(2 * span + width, width)],
    ]
    pairs = [
        (stream_hbm, stream),
        (gain_hbm, gain),
        (lower_hbm, lower),
        (upper_hbm.at[:, columns], upper),
        (boost_hbm.at[:, columns], boost),
        *zip(sources, places),
        (head_gain_hbm, head_gain_ref),
        (gain_two_hbm, gain_ref),
        (index_hbm, index_ref),
        (score_hbm, score_ref),
        (prob_hbm, prob_ref),
        (state_hbm, state_ref),
        (output_hbm, w_out),
        (expert_gate_hbm, w_gate),
        (expert_up_hbm, w_up),
        (expert_down_hbm, w_down),
    ]
    copies = [
        pltpu.make_async_copy(source, place, load_sem.at[i])
        for i, (source, place) in enumerate(pairs)
    ]
    loads = copies[5:9]
    tables = copies[9:14]
    state_load, out_load = copies[14:16]
    expert_loads = copies[16:]
    for load in copies[:14]:
        load.start()
    done = []
    for load in copies[:2]:
        load.wait()
    floats = stream[...].astype(F32)
    scale = lax.rsqrt(jnp.mean(floats * floats, axis=-1, keepdims=True) + epsilon)
    normed = (floats * scale * gain[...]).astype(BF16)
    for d in range(rows):
        chunks[d] = normed[:, d * 2 * feats : (d + 1) * 2 * feats]
    spread[row] = chunks[row]
    pl.semaphore_wait(barrier, len(partners))
    for j, there in enumerate([near, 3 - near, 3 - row]):
        done.append(
            send(
                chunks.at[there],
                spread.at[row],
                chunk_send.at[j],
                chunk_recv.at[row],
                {"ep": there * 2 + core},
            )
        )
    pushes = [
        send(source, place, push_send.at[i], push_recv.at[i], partner)
        for i, (source, place) in enumerate(zip(sources, places))
    ]
    for load in copies[2:5]:
        load.wait()
    low_rank = lax.dot_general(normed, lower[...], nt, preferred_element_type=F32).astype(BF16)
    logit = jnp.dot(low_rank, upper[...], preferred_element_type=F32)
    log_sig = jnp.minimum(logit, 0.0) - jnp.log1p(jnp.exp(-jnp.abs(logit)))
    factor = jnp.exp(log_sig / forgetting_softness - boost[...])

    def fill(first, value):
        for i in range(steps):
            lines[i, first : first + STEP] = value[i * STEP : (i + 1) * STEP]

    def fill_exact(first, value):
        high = value.astype(BF16).astype(F32)
        middle = (value - high).astype(BF16).astype(F32)
        fill(first, high)
        fill(first + STEP, middle)
        fill(first + 2 * STEP, value - high - middle)

    fill_exact(0, factor)
    fill(7 * STEP, jnp.zeros_like(factor))
    line = lax.broadcasted_iota(jnp.int32, spots.shape, 0)
    block = lax.broadcasted_iota(jnp.int32, spots.shape, 1) // KEY_CHANNELS
    band = line // STEP
    kind = (band >= 3).astype(jnp.int32) + (band >= 4).astype(jnp.int32)
    wanted = (block // STEP == kind) & (block % STEP == line % STEP) & (band < 7)
    spots[...] = wanted.astype(F32).astype(BF16)

    cuts = [(0, 2 * span), (2 * span, width), (2 * span + width, width)]
    needs = [(0, 1), (2,), (3,)]

    def cut_of(ref, b, *lead):
        return ref.at[(*lead, slice(None), pl.ds(*cuts[b]))]

    def expect(target, sem):
        pltpu.make_async_remote_copy(
            src_ref=target,
            dst_ref=target,
            send_sem=sem,
            recv_sem=sem,
            device_id=partner,
            device_id_type=MESH,
        ).wait_recv()

    def prepare(b):
        for i in needs[b]:
            loads[i].wait()
            pushes[i].wait_recv()

    def part_of(source, b):
        start, size = cuts[b]
        return jnp.dot(
            spread[source], weights[:, start : start + size], preferred_element_type=F32
        )

    def arrival(there):
        expect(spread.at[there], chunk_recv.at[there])

    def to_near(b):
        start, size = cuts[b]
        near_out[:, start : start + size] = part_of(near, b).astype(BF16)
        done.append(
            send(
                cut_of(near_out, b),
                cut_of(near_in, b),
                near_send.at[b],
                near_recv.at[b],
                {"ep": near * 2 + core},
            )
        )

    def to_inner(b):
        start, size = cuts[b]
        part = part_of(inner_there, b)
        held[:, start : start + size] = part
        mid_out[:, start : start + size] = part.astype(BF16)

        @pl.when(jnp.logical_not(inside))
        def _():
            send(
                cut_of(mid_out, b),
                cut_of(mid_in, b),
                mid_send.at[b],
                mid_recv.at[b],
                {"ep": near * 2 + core},
            )

    slot = jnp.where(inside, 0, 1)

    def to_outer(b):
        start, size = cuts[b]
        far_out[:, start : start + size] = part_of(outer_there, b).astype(BF16)
        done.append(
            send(
                cut_of(far_out, b),
                cut_of(far_in, b, slot),
                far_send.at[b],
                far_recv.at[slot, b],
                {"ep": outer_there * 2 + core},
            )
        )

    def middle_copy(b):
        return pltpu.make_async_remote_copy(
            src_ref=cut_of(mid_out, b),
            dst_ref=cut_of(far_in, b, 0),
            send_sem=mid_send.at[b],
            recv_sem=far_recv.at[0, b],
            device_id={"ep": inner_there * 2 + core},
            device_id_type=MESH,
        )

    def merge(b):
        start, size = cuts[b]

        @pl.when(inside)
        def _():
            expect(cut_of(mid_in, b), mid_recv.at[b])
            merged = held[:, start : start + size] + mid_in[:, start : start + size].astype(F32)
            mid_out[:, start : start + size] = merged.astype(BF16)
            middle_copy(b).start()

        held[:, start : start + size] = part_of(row, b)

    def total_of(b):
        start, size = cuts[b]
        expect(cut_of(near_in, b), near_recv.at[b])
        expect(cut_of(far_in, b, 0), far_recv.at[0, b])
        held[:, start : start + size] += near_in[:, start : start + size].astype(F32) + far_in[
            0, :, start : start + size
        ].astype(F32)

        @pl.when(jnp.logical_not(inside))
        def _():
            expect(cut_of(far_in, b, 1), far_recv.at[1, b])
            held[:, start : start + size] += far_in[1, :, start : start + size].astype(F32)

        return held[:, start : start + size]

    arrival(near)
    prepare(0)
    to_near(0)
    state_load.start()
    arrival(inner_there)
    to_inner(0)
    arrival(outer_there)
    to_outer(0)
    prepare(1)
    to_inner(1)
    to_outer(1)
    to_near(1)
    out_load.start()
    merge(0)
    prepare(2)
    to_inner(2)
    to_outer(2)
    to_near(2)
    for load in expert_loads:
        load.start()
    pushes.append(
        send(expert_down_hbm.at[0], pair_down, push_send.at[4], push_recv.at[4], partner)
    )
    merge(1)
    merge(2)
    total = total_of(0)
    query = (total[:, :span] * KEY_CHANNELS ** (-0.5)).astype(BF16).astype(F32)
    key = total[:, span:].astype(BF16).astype(F32)
    fill(3 * STEP, key)
    fill_exact(4 * STEP, query * factor)
    alike = query * key
    state_load.wait()

    @pl.loop(0, steps)
    def _(i):
        for h in range(heads):
            flat = lines[i, :, h * KEY_CHANNELS : (h + 1) * KEY_CHANNELS].T.astype(BF16)
            turned[i, h] = flat
            wide[h, :, 0 : STEP * KEY_CHANNELS] = jnp.dot(
                flat, spots[:, 2 * STEP * KEY_CHANNELS :], preferred_element_type=F32
            )
        for s in range(STEP):
            sums = []
            for h in range(heads):
                weight = wide[h, :, s * KEY_CHANNELS : (s + 1) * KEY_CHANNELS]
                for g in range(DV // KEY_CHANNELS):
                    start = h * DV + g * KEY_CHANNELS
                    old = state_ref[i * STEP + s, :, start : start + KEY_CHANNELS]
                    sums.append(jnp.sum((weight * old).reshape(-1, 8, KEY_CHANNELS), axis=0))
            read[i * STEP + s] = jnp.concatenate(sums, axis=1)

    def renew(i):
        for h in range(heads):
            wide[h] = jnp.dot(
                turned[i, h], spots[:, : 2 * STEP * KEY_CHANNELS], preferred_element_type=F32
            )
        for s in range(STEP):
            for h in range(heads):
                keep, add = (
                    wide[h, :, (j * STEP + s) * KEY_CHANNELS : (j * STEP + s + 1) * KEY_CHANNELS]
                    for j in range(2)
                )
                for g in range(DV // KEY_CHANNELS):
                    start = h * DV + g * KEY_CHANNELS
                    cut = slice(start, start + KEY_CHANNELS)
                    state_ref[i * STEP + s, :, cut] = (
                        keep * state_ref[i * STEP + s, :, cut]
                        + add * values[i * STEP + s : i * STEP + s + 1, cut]
                    )

    values[...] = total_of(1).astype(BF16).astype(F32)
    readout = jnp.sum(read[...], axis=1)
    gates = total_of(2).astype(BF16).astype(F32)
    silu = gates / (1.0 + jnp.exp(-gates))
    for load in tables:
        load.wait()
    for h in range(heads):
        cut = slice(h * DV, (h + 1) * DV)
        same = jnp.sum(
            alike[:, h * KEY_CHANNELS : (h + 1) * KEY_CHANNELS], axis=-1, keepdims=True
        )
        part = readout[:, cut] + same * values[:, cut]
        mean_sq = jnp.mean(part * part, axis=-1, keepdims=True)
        held[:, cut] = part * lax.rsqrt(mean_sq + epsilon) * head_gain_ref[...] * silu[:, cut]
    gated = held[:, :width].astype(BF16)
    parts = []
    out_load.wait()
    for j, there in enumerate(tps + [tp]):
        cut = pl.ds(pl.multiple_of(there * width, 128), width)
        part = jnp.dot(gated, w_out[:, cut], preferred_element_type=F32)
        if j < m - 1:
            part_out[j] = part.astype(BF16)
            parts.append(
                send(part_out.at[j], part_in.at[j], part_send.at[j], part_recv.at[j], {"tp": there})
            )

    index = index_ref[...]
    group = index[0:1] // 2
    band = lax.broadcasted_iota(jnp.int32, (8, seqs), 0)
    one_hot = (band == group).astype(F32)
    earlier = lax.broadcasted_iota(jnp.int32, (seqs, seqs), 0) < lax.broadcasted_iota(
        jnp.int32, (seqs, seqs), 1
    )
    counts = jnp.dot(one_hot, earlier.astype(F32), preferred_element_type=F32)
    rank = jnp.sum(counts * one_hot, axis=0, keepdims=True).astype(jnp.int32)
    slot_line = lax.broadcasted_iota(jnp.int32, (GROUPS * capacity, seqs), 0)
    placing = (slot_line == group * capacity + rank).astype(F32)
    scores = jnp.exp(score_ref[...])
    shares = scores / jnp.sum(scores, axis=0, keepdims=True) * prob_ref[...]
    place_line = lax.broadcasted_iota(jnp.int32, (128, seqs), 0)
    table = jnp.zeros((128, seqs), F32)
    for k in range(index.shape[0]):
        table += jnp.where(place_line == lax.rem(index[k : k + 1], 2), shares[k : k + 1], 0.0)
    shares_out[...] = lax.dot_general(
        placing, table, nt, preferred_element_type=F32, precision=lax.Precision.HIGHEST
    ).reshape(GROUPS, capacity, 128)
    placing = placing.astype(BF16)

    for z in zs:
        done.append(
            send(
                shares_out.at[z],
                shares_in.at[row],
                share_send.at[z],
                share_recv.at[row],
                {"ep": z * 2 + core},
            )
        )
    shares_in[row] = shares_out[row]
    renew(0)
    own_cut = pl.ds(pl.multiple_of(tp * width, 128), width)
    total = part + stream[:, own_cut].astype(F32)
    for j in (1, 2, 0):
        parts[j].wait_recv()
        total = total + part_in[j].astype(F32)
    mixed = total.astype(BF16)
    slots = jnp.dot(placing, mixed, preferred_element_type=F32)
    slots_out[...] = slots.reshape(GROUPS, capacity, width).astype(BF16)
    for z in zs:
        done.append(
            send(
                slots_out.at[z],
                arrived.at[tp, core, row],
                slot_send.at[z],
                slot_recv.at[row],
                {"ep": z * 2 + core},
            )
        )
    arrived[tp, core, row] = slots_out[row]

    def swap(t, z):
        done.append(
            send(
                arrived.at[t, core, z],
                arrived.at[t, core, z],
                swap_send.at[t, z],
                swap_recv.at[t, z],
                {"ep": other},
            )
        )

    def join(z):
        for t in tps:
            done.append(
                send(
                    arrived.at[tp, core, z],
                    arrived.at[tp, core, z],
                    join_send.at[t, z],
                    join_recv.at[tp, z],
                    {"tp": t},
                )
            )
        swap(tp, z)

    def relay(z):
        for t in (tps[1], tps[2], tps[0]):
            expect(arrived.at[t, core, z], join_recv.at[t, z])
            swap(t, z)

    order = [row] + zs[::-1]
    join(row)
    renew(1)
    expect(arrived.at[tp, core, order[1]], slot_recv.at[order[1]])
    join(order[1])
    expect(arrived.at[tp, core, order[2]], slot_recv.at[order[2]])
    join(order[2])
    relay(order[0])
    expect(arrived.at[tp, core, order[3]], slot_recv.at[order[3]])
    join(order[3])
    renew(2)
    relay(order[1])
    relay(order[2])
    for load in expert_loads:
        load.wait()

    tokens_held = n * capacity
    square = jnp.zeros((tokens_held, 1), F32)
    gate_pre = jnp.zeros((tokens_held, inner), F32)
    up_pre = jnp.zeros((tokens_held, inner), F32)
    for j, t in enumerate([tp, tps[1], tps[2], tps[0]]):
        if j == 1:
            relay(order[3])
        for z in order:
            expect(arrived.at[t, 1 - core, z], swap_recv.at[t, z])
        cut = pl.ds(pl.multiple_of(t * width, 128), width)
        tokens = arrived[t].astype(F32).reshape(tokens_held, width)
        square += jnp.sum(tokens * tokens, axis=-1, keepdims=True)
        scaled = (tokens * gain_ref[:, cut]).astype(BF16)
        gate_pre += lax.dot_general(scaled, w_gate[0, :, cut], nt, preferred_element_type=F32)
        up_pre += lax.dot_general(scaled, w_up[0, :, cut], nt, preferred_element_type=F32)
    scale = lax.rsqrt(square / (m * width) + epsilon)
    gate_pre *= scale
    up_pre *= scale
    hidden_out[...] = (
        (gate_pre / (1.0 + jnp.exp(-gate_pre)) * up_pre).astype(BF16).reshape(2, half, inner)
    )
    for j, t in enumerate(tps):
        for c in range(2):
            done.append(
                send(
                    hidden_out.at[c],
                    hidden_in.at[core, tp],
                    hid_send.at[2 * j + c],
                    hid_recv.at[core, tp],
                    {"tp": t, "ep": row * 2 + c},
                )
            )
    done.append(
        send(
            hidden_out.at[1 - core],
            hidden_in.at[core, tp],
            hid_send.at[2 * m - 2],
            hid_recv.at[core, tp],
            {"ep": other},
        )
    )
    hidden_in[core, tp] = hidden_out[core]
    renew(3)
    pushes[4].wait_recv()
    own_sum = jnp.zeros((half, width), F32)
    pair_sum = jnp.zeros((half, width), F32)
    for j, t in enumerate([tp, tps[1], tps[2], tps[0]]):
        band = pl.ds(pl.multiple_of(t * inner, 128), inner)
        if j > 0:
            expect(hidden_in.at[core, t], hid_recv.at[core, t])
        own_sum += jnp.dot(hidden_in[core, t], w_down[0, band, :], preferred_element_type=F32)
        expect(hidden_in.at[1 - core, t], hid_recv.at[1 - core, t])
        pair_sum += jnp.dot(hidden_in[1 - core, t], pair_down[band, :], preferred_element_type=F32)
    for z in zs:
        expect(shares_in.at[z], share_recv.at[z])
    share = shares_in[...].reshape(half, 128)
    which = lax.broadcasted_iota(jnp.int32, (half, 128), 1)
    own_share = jnp.sum(jnp.where(which == core, share, 0.0), axis=1, keepdims=True)
    pair_share = jnp.sum(jnp.where(which == 1 - core, share, 0.0), axis=1, keepdims=True)
    outputs = own_share * own_sum.astype(BF16).astype(F32) + pair_share * pair_sum.astype(
        BF16
    ).astype(F32)
    ready[...] = outputs.reshape(rows, capacity, width).astype(BF16)
    for z in zs:
        done.append(
            send(
                ready.at[z],
                returned.at[row],
                back_send.at[z],
                back_recv.at[row],
                {"ep": z * 2 + core},
            )
        )
    returned[row] = ready[row]
    for z in zs[::-1]:
        expect(returned.at[z], back_recv.at[z])
    mixture = lax.dot_general(
        placing,
        returned[...].reshape(half, width),
        (((0,), (0,)), ((), ())),
        preferred_element_type=F32,
    )
    out_ref[...] = (mixed.astype(F32) + mixture).astype(BF16)
    for copy in parts + done + pushes:
        copy.wait_send()
    for b in range(3):
        middle_copy(b).wait_send()


def fused(
    stream,
    previous_state,
    mixer_norm_gain,
    query_matrix,
    key_matrix,
    value_matrix,
    output_gate_weight,
    decay_lower_factor,
    decay_upper_factor,
    forgetting_boost,
    head_norm_gain,
    output_matrix,
    mixture_norm_gain,
    expert_gate_weight,
    expert_up_weight,
    expert_down_weight,
    expert_index_table,
    expert_scores_within,
    group_probability,
):
    n = lax.axis_size("ep")
    m = lax.axis_size("tp")
    seqs, model = stream.shape
    width = previous_state.shape[2]
    span = width // DV * KEY_CHANNELS
    feats = query_matrix.shape[0]
    rank = decay_lower_factor.shape[1]
    steps = seqs // STEP
    total = 2 * span + 2 * width
    rows = n // 2
    inner = expert_gate_weight.shape[1]
    capacity = 2 * seqs * expert_index_table.shape[1] // n
    lines = 8 * STEP
    dma = pltpu.SemaphoreType.DMA
    vmem = pl.BlockSpec(memory_space=pltpu.VMEM)
    hbm = pl.BlockSpec(memory_space=pltpu.HBM)
    operands = (
        stream,
        mixer_norm_gain.reshape(1, model),
        query_matrix,
        key_matrix,
        value_matrix,
        output_gate_weight,
        decay_lower_factor.T,
        decay_upper_factor,
        forgetting_boost,
        head_norm_gain.reshape(1, DV),
        mixture_norm_gain.reshape(1, model),
        expert_index_table.T,
        expert_scores_within.T,
        group_probability.reshape(1, seqs),
        previous_state,
        output_matrix,
        expert_gate_weight,
        expert_up_weight,
        expert_down_weight,
    )
    new_state, new_stream = pl.pallas_call(
        functools.partial(layer_kernel, n, m),
        name="layer",
        out_shape=(
            pltpu.VMEM(previous_state.shape, F32),
            jax.ShapeDtypeStruct((seqs, width), BF16),
        ),
        in_specs=[hbm] * len(operands),
        out_specs=(vmem, vmem),
        scratch_shapes=[
            pltpu.VMEM((seqs, model), BF16),
            pltpu.VMEM((1, model), F32),
            pltpu.VMEM((2 * feats, total), BF16),
            pltpu.VMEM((rank, model), BF16),
            pltpu.VMEM((rank, span), BF16),
            pltpu.VMEM((seqs, span), F32),
            pltpu.VMEM((1, DV), F32),
            pltpu.VMEM((1, model), F32),
            pltpu.VMEM(expert_index_table.shape[::-1], jnp.int32),
            pltpu.VMEM(expert_scores_within.shape[::-1], F32),
            pltpu.VMEM((1, seqs), F32),
            pltpu.VMEM(output_matrix.shape, BF16),
            pltpu.VMEM(expert_gate_weight.shape, BF16),
            pltpu.VMEM(expert_up_weight.shape, BF16),
            pltpu.VMEM(expert_down_weight.shape, BF16),
            pltpu.VMEM(expert_down_weight.shape[1:], BF16),
            pltpu.VMEM((rows, seqs, 2 * feats), BF16),
            pltpu.VMEM((rows, seqs, 2 * feats), BF16),
            pltpu.VMEM((seqs, total), BF16),
            pltpu.VMEM((seqs, total), BF16),
            pltpu.VMEM((seqs, total), BF16),
            pltpu.VMEM((seqs, total), BF16),
            pltpu.VMEM((seqs, total), BF16),
            pltpu.VMEM((2, seqs, total), BF16),
            pltpu.VMEM((seqs, total), F32),
            pltpu.VMEM((steps, lines, span), F32),
            pltpu.VMEM((steps, width // DV, KEY_CHANNELS, lines), BF16),
            pltpu.VMEM((lines, 3 * STEP * KEY_CHANNELS), BF16),
            pltpu.VMEM((width // DV, KEY_CHANNELS, 2 * STEP * KEY_CHANNELS), F32),
            pltpu.VMEM((seqs, width), F32),
            pltpu.VMEM((seqs, 8, width), F32),
            pltpu.VMEM((m - 1, seqs, width), BF16),
            pltpu.VMEM((m - 1, seqs, width), BF16),
            pltpu.VMEM((GROUPS, capacity, width), BF16),
            pltpu.VMEM((GROUPS, capacity, 128), F32),
            pltpu.VMEM((GROUPS, capacity, 128), F32),
            pltpu.VMEM((m, 2, rows, capacity, width), BF16),
            pltpu.VMEM((2, rows * capacity, inner), BF16),
            pltpu.VMEM((2, m, rows * capacity, inner), BF16),
            pltpu.VMEM((rows, capacity, width), BF16),
            pltpu.VMEM((rows, capacity, width), BF16),
            dma((len(operands),)),
            dma((5,)),
            dma((5,)),
            dma((rows,)),
            dma((rows,)),
            dma((3,)),
            dma((3,)),
            dma((3,)),
            dma((3,)),
            dma((3,)),
            dma((2, 3)),
            dma((m - 1,)),
            dma((m - 1,)),
            dma((rows,)),
            dma((rows,)),
            dma((rows,)),
            dma((rows,)),
            dma((m, rows)),
            dma((m, rows)),
            dma((m, rows)),
            dma((m, rows)),
            dma((2 * m - 1,)),
            dma((2, m)),
            dma((rows,)),
            dma((rows,)),
        ],
        compiler_params=pltpu.CompilerParams(
            collective_id=0, has_side_effects=True, vmem_limit_bytes=GRANT * 2**20
        ),
        cost_estimate=pl.CostEstimate(
            flops=COST, bytes_accessed=4 * previous_state.size, transcendentals=0
        ),
    )(*(pltpu.with_memory_space_constraint(a, pltpu.HBM) for a in operands))
    return (new_stream, new_state)


def on_device(*arrays):
    stream, state = arrays[0], arrays[1]
    experts_held, route_count = arrays[13].shape[0], arrays[16].shape[1]
    n = lax.axis_size("ep")
    whole_heads = state.shape[2] % DV == 0
    pair_routed = experts_held == 1 and n == GROUPS * route_count and route_count == 2
    boxed = n == 8 and lax.axis_size("tp") == 4
    full_tiles = stream.shape[0] % 16 == 0 and stream.shape[1] == state.shape[2] * lax.axis_size("tp")
    if whole_heads and pair_routed and full_tiles and boxed:
        return fused(*arrays)
    return general(*arrays)


def solution(mesh):
    placed = (
        P("ep", None),
        P("ep", None, "tp"),
        P(),
        P("ep", None),
        P("ep", None),
        P("ep", "tp"),
        P("ep", "tp"),
        P(),
        P(),
        P("ep", None),
        P(),
        P("tp", None),
        P(),
        P("ep", "tp", None),
        P("ep", "tp", None),
        P("ep", None, "tp"),
        P("ep", None),
        P("ep", None),
        P("ep"),
    )
    return jax.shard_map(
        on_device,
        mesh=mesh,
        in_specs=placed,
        out_specs=(P("ep", "tp"), P("ep", None, "tp")),
        check_vma=False,
    )
```

```python
import functools

import jax
import jax.numpy as jnp
from jax import lax
from jax.experimental import pallas as pl
from jax.experimental.pallas import tpu as pltpu
from jax.sharding import PartitionSpec as P

HEAD_TOTAL = 16
KEY_CHANNELS = 128
DV = 256
GROUPS = 4
STEP = 4
COST = 20_000_000_000
GRANT = 40
F32 = jnp.float32
BF16 = jnp.bfloat16
MESH = pl.DeviceIdType.MESH

epsilon = 1e-06
forgetting_softness = 16.0


def rms_scaled(values, gain_vec):
    floats = values.astype(jnp.float32)
    scaled = floats * lax.rsqrt(jnp.mean(floats * floats, axis=-1, keepdims=True) + epsilon)
    return (scaled * gain_vec).astype(jnp.bfloat16)


def general(
    stream,
    previous_state,
    mixer_norm_gain,
    query_matrix,
    key_matrix,
    value_matrix,
    output_gate_weight,
    decay_lower_factor,
    decay_upper_factor,
    forgetting_boost,
    head_norm_gain,
    output_matrix,
    mixture_norm_gain,
    expert_gate_weight,
    expert_up_weight,
    expert_down_weight,
    expert_index_table,
    expert_scores_within,
    group_probability,
):
    seq_count, model_width = stream.shape
    value_local = previous_state.shape[2]
    head_count = max(1, value_local // DV)
    head_width = min(value_local, DV)
    tp_index = lax.axis_index("tp")
    leading_head = tp_index * value_local // DV
    value_start = tp_index * value_local % DV
    key_column_span = head_count * KEY_CHANNELS
    normed = rms_scaled(stream, mixer_norm_gain)
    own_query = lax.dynamic_slice_in_dim(
        query_matrix, leading_head * KEY_CHANNELS, key_column_span, 1
    )
    own_key = lax.dynamic_slice_in_dim(key_matrix, leading_head * KEY_CHANNELS, key_column_span, 1)
    spread = lax.all_to_all(normed, "ep", split_axis=1, concat_axis=0, tiled=True)
    joined = jnp.concatenate([own_query, own_key, value_matrix, output_gate_weight], axis=1)
    summed = lax.psum_scatter(
        jnp.dot(spread, joined, preferred_element_type=jnp.float32),
        "ep",
        scatter_dimension=0,
        tiled=True,
    )
    query_sum = summed[:, :key_column_span]
    key_sum = summed[:, key_column_span : 2 * key_column_span]
    value_sum = summed[:, 2 * key_column_span : 2 * key_column_span + value_local]
    gate_sum = summed[:, 2 * key_column_span + value_local :]
    queries = (query_sum * KEY_CHANNELS ** (-0.5)).astype(jnp.bfloat16)
    key_rows = key_sum.astype(jnp.bfloat16)
    value_rows = value_sum.astype(jnp.bfloat16)
    gate_rows = gate_sum.astype(jnp.bfloat16)
    low_rank = jnp.dot(normed, decay_lower_factor, preferred_element_type=jnp.float32).astype(
        jnp.bfloat16
    )
    local_expand_matrix = lax.dynamic_slice_in_dim(
        decay_upper_factor, leading_head * KEY_CHANNELS, key_column_span, 1
    )
    forgetting_logit = jnp.dot(low_rank, local_expand_matrix, preferred_element_type=jnp.float32)
    request_boost = lax.dynamic_slice_in_dim(
        forgetting_boost, leading_head * KEY_CHANNELS, key_column_span, 1
    )
    forgetting_lograte = jax.nn.log_sigmoid(forgetting_logit) / forgetting_softness - request_boost
    factor = (
        jnp.exp(forgetting_lograte)
        .reshape(seq_count, head_count, KEY_CHANNELS)
        .transpose(0, 2, 1)[..., None]
    )
    state_four = previous_state.reshape(seq_count, KEY_CHANNELS, head_count, head_width)
    key_part = (
        key_rows.astype(jnp.float32)
        .reshape(seq_count, head_count, KEY_CHANNELS)
        .transpose(0, 2, 1)[..., None]
    )
    value_part = value_rows.astype(jnp.float32).reshape(seq_count, 1, head_count, head_width)
    updated = factor * state_four + key_part * value_part
    query_part = (
        queries.astype(jnp.float32).reshape(seq_count, head_count, KEY_CHANNELS).transpose(0, 2, 1)
    )
    readout = jnp.einsum("skh,skhv->shv", query_part, updated, precision=lax.Precision.HIGHEST)
    square_sums = jnp.sum(readout * readout, axis=-1)
    norm_table = lax.dynamic_update_slice(
        jnp.zeros((seq_count, HEAD_TOTAL), jnp.float32), square_sums, (jnp.int32(0), leading_head)
    )
    totals = lax.psum(norm_table, "tp")
    own_totals = lax.dynamic_slice_in_dim(totals, leading_head, head_count, 1)
    mean_sq = own_totals[..., None] / DV
    own_gain = lax.dynamic_slice_in_dim(head_norm_gain, value_start, head_width, 0)
    gate_part = jax.nn.silu(
        gate_rows.astype(jnp.float32).reshape(seq_count, head_count, head_width)
    )
    gated_rows = (
        (readout * lax.rsqrt(mean_sq + epsilon) * own_gain * gate_part)
        .reshape(seq_count, value_local)
        .astype(jnp.bfloat16)
    )
    partial_out = jnp.dot(gated_rows, output_matrix, preferred_element_type=jnp.float32)
    mixer_sum = lax.psum(partial_out.astype(jnp.bfloat16), "tp").astype(jnp.float32)
    blended_tokens = (stream.astype(jnp.float32) + mixer_sum).astype(jnp.bfloat16)
    normed_two = rms_scaled(blended_tokens, mixture_norm_gain)
    ep_count = lax.axis_size("ep")
    local_experts = expert_gate_weight.shape[0]
    experts_all = ep_count * local_experts
    route_count = expert_index_table.shape[1]
    capacity = 2 * seq_count * route_count // experts_all
    slot_count = experts_all * capacity
    flat_ids = expert_index_table.reshape(seq_count * route_count)
    one_hot = (flat_ids[:, None] == jnp.arange(experts_all, dtype=jnp.int32)[None, :]).astype(
        jnp.int32
    )
    rank_in = jnp.sum(one_hot * (jnp.cumsum(one_hot, axis=0) - 1), axis=1)
    place_lookup = flat_ids * capacity + rank_in
    placing = (place_lookup[:, None] == jnp.arange(slot_count, dtype=jnp.int32)[None, :]).astype(
        jnp.float32
    )
    placing = placing.reshape(seq_count, route_count, slot_count)
    logit_exp = jnp.exp(expert_scores_within)
    weights = logit_exp / jnp.sum(logit_exp, axis=-1, keepdims=True) * group_probability[:, None]
    combine = jnp.einsum("sk,skc->sc", weights, placing, precision=lax.Precision.HIGHEST)
    dispatch = jnp.sum(placing, axis=1).astype(jnp.bfloat16)
    outgoing = jnp.einsum("sc,sd->cd", dispatch, normed_two, preferred_element_type=jnp.float32)
    outgoing = outgoing.astype(jnp.bfloat16).reshape(experts_all, capacity, model_width)
    width_local = expert_down_weight.shape[2]
    arrived = lax.all_to_all(outgoing, "ep", split_axis=0, concat_axis=0, tiled=True)
    held_slots = arrived.shape[1]
    grouped = arrived.reshape(ep_count, local_experts, held_slots, model_width)
    gate_pre = jnp.einsum(
        "sxcd,xfd->sxcf", grouped, expert_gate_weight, preferred_element_type=jnp.float32
    )
    up_pre = jnp.einsum(
        "sxcd,xfd->sxcf", grouped, expert_up_weight, preferred_element_type=jnp.float32
    )
    hidden = (jax.nn.silu(gate_pre) * up_pre).astype(jnp.bfloat16)
    outputs = jnp.einsum(
        "sxcf,xfd->sxcd",
        lax.all_gather(hidden, "tp", axis=3, tiled=True),
        expert_down_weight,
        preferred_element_type=jnp.float32,
    )
    ready_rows = outputs.astype(jnp.bfloat16).reshape(
        ep_count * local_experts, held_slots, width_local
    )
    returned = lax.all_to_all(ready_rows, "ep", split_axis=0, concat_axis=0, tiled=True)
    mixture = jnp.dot(
        combine,
        returned.reshape(slot_count, width_local).astype(jnp.float32),
        precision=lax.Precision.HIGHEST,
    )
    own_mixed = lax.dynamic_slice_in_dim(blended_tokens, tp_index * width_local, width_local, 1)
    new_stream = (own_mixed.astype(jnp.float32) + mixture).astype(jnp.bfloat16)
    return (new_stream, updated.reshape(seq_count, KEY_CHANNELS, value_local))


def send(source, target, send_sem, recv_sem, partner):
    copy = pltpu.make_async_remote_copy(
        src_ref=source,
        dst_ref=target,
        send_sem=send_sem,
        recv_sem=recv_sem,
        device_id=partner,
        device_id_type=MESH,
    )
    copy.start()
    return copy


def layer_kernel(
    n,
    m,
    stream_hbm,
    gain_hbm,
    query_hbm,
    key_hbm,
    value_hbm,
    gate_hbm,
    lower_hbm,
    upper_hbm,
    boost_hbm,
    head_gain_hbm,
    gain_two_hbm,
    index_hbm,
    score_hbm,
    prob_hbm,
    state_hbm,
    output_hbm,
    expert_gate_hbm,
    expert_up_hbm,
    expert_down_hbm,
    state_ref,
    out_ref,
    stream,
    gain,
    weights,
    lower,
    upper,
    boost,
    head_gain_ref,
    gain_ref,
    index_ref,
    score_ref,
    prob_ref,
    w_out,
    w_in,
    w_down,
    pair_down,
    chunks,
    spread,
    near_out,
    near_in,
    mid_out,
    mid_in,
    far_out,
    far_in,
    held,
    lines,
    turned,
    spots,
    wide,
    values,
    read,
    part_out,
    part_in,
    slots_out,
    shares_out,
    shares_in,
    arrived,
    hidden_out,
    hidden_in,
    ready,
    returned,
    load_sem,
    push_send,
    push_recv,
    chunk_send,
    chunk_recv,
    near_send,
    near_recv,
    mid_send,
    mid_recv,
    far_send,
    far_recv,
    part_send,
    part_recv,
    slot_send,
    slot_recv,
    share_send,
    share_recv,
    join_send,
    join_recv,
    swap_send,
    swap_recv,
    hid_send,
    hid_recv,
    back_send,
    back_recv,
):
    me = lax.axis_index("ep")
    tp = lax.axis_index("tp")
    core = lax.rem(me, 2)
    row = me // 2
    rows = n // 2
    seqs = stream.shape[0]
    feats = query_hbm.shape[0]
    span = boost.shape[1]
    width = value_hbm.shape[1]
    heads = width // DV
    steps = seqs // STEP
    capacity = slots_out.shape[1]
    half = rows * capacity
    inner = w_in.shape[1]
    nt = (((1,), (1,)), ((), ()))
    side = row // 2
    inside = lax.rem(row, 2) != side
    near = row + 1 - 2 * lax.rem(row, 2)
    inner_there = 2 - side
    outer_there = 3 - 3 * side
    other = me + 1 - 2 * core
    partner = {"ep": other}
    zs = [3 - row, 3 - near, near]
    tps = [m - 1 - tp, tp + 1 - 2 * lax.rem(tp, 2), lax.rem(tp + 2, m)]
    partners = (
        [partner]
        + [{"ep": z * 2 + core} for z in zs]
        + [{"tp": t} for t in tps]
        + [{"tp": t, "ep": other} for t in tps]
    )
    barrier = pltpu.get_barrier_semaphore()
    for there in partners:
        pl.semaphore_signal(barrier, inc=1, device_id=there, device_id_type=MESH)

    columns = pl.ds(pl.multiple_of(tp * span, 128), span)
    mine = pl.ds(pl.multiple_of(core * feats, 128), feats)
    sources = [query_hbm.at[:, columns], key_hbm.at[:, columns], value_hbm, gate_hbm]
    places = [
        weights.at[mine, pl.ds(0, span)],
        weights.at[mine, pl.ds(span, span)],
        weights.at[mine, pl.ds(2 * span, width)],
        weights.at[mine, pl.ds(2 * span + width, width)],
    ]
    pairs = [
        (stream_hbm, stream),
        (gain_hbm, gain),
        (lower_hbm, lower),
        (upper_hbm.at[:, columns], upper),
        (boost_hbm.at[:, columns], boost),
        *zip(sources, places),
        (head_gain_hbm, head_gain_ref),
        (gain_two_hbm, gain_ref),
        (index_hbm, index_ref),
        (score_hbm, score_ref),
        (prob_hbm, prob_ref),
        (state_hbm, state_ref),
        (output_hbm, w_out),
        (expert_gate_hbm.at[0], w_in.at[0]),
        (expert_up_hbm.at[0], w_in.at[1]),
        (expert_down_hbm, w_down),
    ]
    copies = [
        pltpu.make_async_copy(source, place, load_sem.at[i])
        for i, (source, place) in enumerate(pairs)
    ]
    loads = copies[5:9]
    tables = copies[9:14]
    state_load, out_load = copies[14:16]
    expert_loads = copies[16:]
    for load in copies[:14]:
        load.start()
    done = []
    for load in copies[:2]:
        load.wait()
    floats = stream[...].astype(F32)
    scale = lax.rsqrt(jnp.mean(floats * floats, axis=-1, keepdims=True) + epsilon)
    normed = (floats * scale * gain[...]).astype(BF16)
    for d in range(rows):
        chunks[d] = normed[:, d * 2 * feats : (d + 1) * 2 * feats]
    spread[row] = chunks[row]
    pl.semaphore_wait(barrier, len(partners))
    for j, there in enumerate([near, 3 - near, 3 - row]):
        done.append(
            send(
                chunks.at[there],
                spread.at[row],
                chunk_send.at[j],
                chunk_recv.at[row],
                {"ep": there * 2 + core},
            )
        )

    def push(i):
        pushes.append(
            send(sources[i], places[i], push_send.at[i], push_recv.at[i], partner)
        )

    pushes = []
    for i in range(3):
        push(i)
    for load in copies[2:5]:
        load.wait()
    low_rank = lax.dot_general(normed, lower[...], nt, preferred_element_type=F32).astype(BF16)
    logit = jnp.dot(low_rank, upper[...], preferred_element_type=F32)
    log_sig = jnp.minimum(logit, 0.0) - jnp.log1p(jnp.exp(-jnp.abs(logit)))
    factor = jnp.exp(log_sig / forgetting_softness - boost[...])

    def fill(first, value):
        for i in range(steps):
            lines[i, first : first + STEP] = value[i * STEP : (i + 1) * STEP]

    def fill_exact(first, value):
        high = value.astype(BF16).astype(F32)
        middle = (value - high).astype(BF16).astype(F32)
        fill(first, high)
        fill(first + STEP, middle)
        fill(first + 2 * STEP, value - high - middle)

    fill_exact(0, factor)
    fill(7 * STEP, jnp.zeros_like(factor))
    line = lax.broadcasted_iota(jnp.int32, spots.shape, 0)
    block = lax.broadcasted_iota(jnp.int32, spots.shape, 1) // KEY_CHANNELS
    band = line // STEP
    kind = (band >= 3).astype(jnp.int32) + (band >= 4).astype(jnp.int32)
    wanted = (block // STEP == kind) & (block % STEP == line % STEP) & (band < 7)
    spots[...] = wanted.astype(F32).astype(BF16)

    cuts = [(0, 2 * span), (2 * span, width), (2 * span + width, width)]
    needs = [(0, 1), (2,), (3,)]

    def cut_of(ref, b, *lead):
        return ref.at[(*lead, slice(None), pl.ds(*cuts[b]))]

    def expect(target, sem):
        pltpu.make_async_remote_copy(
            src_ref=target,
            dst_ref=target,
            send_sem=sem,
            recv_sem=sem,
            device_id=partner,
            device_id_type=MESH,
        ).wait_recv()

    def prepare(b):
        for i in needs[b]:
            loads[i].wait()
            pushes[i].wait_recv()

    def part_of(source, b):
        start, size = cuts[b]
        return jnp.dot(
            spread[source], weights[:, start : start + size], preferred_element_type=F32
        )

    def arrival(there):
        expect(spread.at[there], chunk_recv.at[there])

    def to_near(b):
        start, size = cuts[b]
        near_out[:, start : start + size] = part_of(near, b).astype(BF16)
        done.append(
            send(
                cut_of(near_out, b),
                cut_of(near_in, b),
                near_send.at[b],
                near_recv.at[b],
                {"ep": near * 2 + core},
            )
        )

    def to_inner(b):
        start, size = cuts[b]
        part = part_of(inner_there, b)
        held[:, start : start + size] = part
        mid_out[:, start : start + size] = part.astype(BF16)

        @pl.when(jnp.logical_not(inside))
        def _():
            send(
                cut_of(mid_out, b),
                cut_of(mid_in, b),
                mid_send.at[b],
                mid_recv.at[b],
                {"ep": near * 2 + core},
            )

    slot = jnp.where(inside, 0, 1)

    def to_outer(b):
        start, size = cuts[b]
        far_out[:, start : start + size] = part_of(outer_there, b).astype(BF16)
        done.append(
            send(
                cut_of(far_out, b),
                cut_of(far_in, b, slot),
                far_send.at[b],
                far_recv.at[slot, b],
                {"ep": outer_there * 2 + core},
            )
        )

    def middle_copy(b):
        return pltpu.make_async_remote_copy(
            src_ref=cut_of(mid_out, b),
            dst_ref=cut_of(far_in, b, 0),
            send_sem=mid_send.at[b],
            recv_sem=far_recv.at[0, b],
            device_id={"ep": inner_there * 2 + core},
            device_id_type=MESH,
        )

    def merge(b):
        start, size = cuts[b]

        @pl.when(inside)
        def _():
            expect(cut_of(mid_in, b), mid_recv.at[b])
            merged = held[:, start : start + size] + mid_in[:, start : start + size].astype(F32)
            mid_out[:, start : start + size] = merged.astype(BF16)
            middle_copy(b).start()

        held[:, start : start + size] = part_of(row, b)

    def total_of(b):
        start, size = cuts[b]
        expect(cut_of(near_in, b), near_recv.at[b])
        expect(cut_of(far_in, b, 0), far_recv.at[0, b])
        held[:, start : start + size] += near_in[:, start : start + size].astype(F32) + far_in[
            0, :, start : start + size
        ].astype(F32)

        @pl.when(jnp.logical_not(inside))
        def _():
            expect(cut_of(far_in, b, 1), far_recv.at[1, b])
            held[:, start : start + size] += far_in[1, :, start : start + size].astype(F32)

        return held[:, start : start + size]

    arrival(near)
    prepare(0)
    to_near(0)
    state_load.start()
    arrival(inner_there)
    to_inner(0)
    arrival(outer_there)
    to_outer(0)
    push(3)
    prepare(1)
    to_inner(1)
    to_outer(1)
    to_near(1)
    out_load.start()
    merge(0)
    prepare(2)
    to_inner(2)
    to_outer(2)
    to_near(2)
    for load in expert_loads:
        load.start()
    pushes.append(
        send(expert_down_hbm.at[0], pair_down, push_send.at[4], push_recv.at[4], partner)
    )
    merge(1)
    merge(2)
    total = total_of(0)
    query = (total[:, :span] * KEY_CHANNELS ** (-0.5)).astype(BF16).astype(F32)
    key = total[:, span:].astype(BF16).astype(F32)
    fill(3 * STEP, key)
    fill_exact(4 * STEP, query * factor)
    alike = query * key
    state_load.wait()

    @pl.loop(0, steps)
    def _(i):
        for h in range(heads):
            flat = lines[i, :, h * KEY_CHANNELS : (h + 1) * KEY_CHANNELS].T.astype(BF16)
            turned[i, h] = flat
            wide[h, :, 0 : STEP * KEY_CHANNELS] = jnp.dot(
                flat, spots[:, 2 * STEP * KEY_CHANNELS :], preferred_element_type=F32
            )
        for s in range(STEP):
            sums = []
            for h in range(heads):
                weight = wide[h, :, s * KEY_CHANNELS : (s + 1) * KEY_CHANNELS]
                for g in range(DV // KEY_CHANNELS):
                    start = h * DV + g * KEY_CHANNELS
                    old = state_ref[i * STEP + s, :, start : start + KEY_CHANNELS]
                    sums.append(jnp.sum((weight * old).reshape(-1, 8, KEY_CHANNELS), axis=0))
            read[i * STEP + s] = jnp.concatenate(sums, axis=1)

    def renew(i):
        for h in range(heads):
            wide[h] = jnp.dot(
                turned[i, h], spots[:, : 2 * STEP * KEY_CHANNELS], preferred_element_type=F32
            )
        for s in range(STEP):
            for h in range(heads):
                keep, add = (
                    wide[h, :, (j * STEP + s) * KEY_CHANNELS : (j * STEP + s + 1) * KEY_CHANNELS]
                    for j in range(2)
                )
                for g in range(DV // KEY_CHANNELS):
                    start = h * DV + g * KEY_CHANNELS
                    cut = slice(start, start + KEY_CHANNELS)
                    state_ref[i * STEP + s, :, cut] = (
                        keep * state_ref[i * STEP + s, :, cut]
                        + add * values[i * STEP + s : i * STEP + s + 1, cut]
                    )

    values[...] = total_of(1).astype(BF16).astype(F32)
    readout = jnp.sum(read[...], axis=1)
    gates = total_of(2).astype(BF16).astype(F32)
    silu = gates / (1.0 + jnp.exp(-gates))
    for load in tables:
        load.wait()
    for h in range(heads):
        cut = slice(h * DV, (h + 1) * DV)
        same = jnp.sum(
            alike[:, h * KEY_CHANNELS : (h + 1) * KEY_CHANNELS], axis=-1, keepdims=True
        )
        part = readout[:, cut] + same * values[:, cut]
        mean_sq = jnp.mean(part * part, axis=-1, keepdims=True)
        held[:, cut] = part * lax.rsqrt(mean_sq + epsilon) * head_gain_ref[...] * silu[:, cut]
    gated = held[:, :width].astype(BF16)
    parts = []
    out_load.wait()
    for j, there in enumerate(tps + [tp]):
        cut = pl.ds(pl.multiple_of(there * width, 128), width)
        part = jnp.dot(gated, w_out[:, cut], preferred_element_type=F32)
        if j < m - 1:
            part_out[j] = part.astype(BF16)
            parts.append(
                send(part_out.at[j], part_in.at[j], part_send.at[j], part_recv.at[j], {"tp": there})
            )

    index = index_ref[...]
    group = index[0:1] // 2
    band = lax.broadcasted_iota(jnp.int32, (8, seqs), 0)
    one_hot = (band == group).astype(F32)
    earlier = lax.broadcasted_iota(jnp.int32, (seqs, seqs), 0) < lax.broadcasted_iota(
        jnp.int32, (seqs, seqs), 1
    )
    counts = jnp.dot(one_hot, earlier.astype(F32), preferred_element_type=F32)
    rank = jnp.sum(counts * one_hot, axis=0, keepdims=True).astype(jnp.int32)
    slot_line = lax.broadcasted_iota(jnp.int32, (GROUPS * capacity, seqs), 0)
    placing = (slot_line == group * capacity + rank).astype(F32)
    scores = jnp.exp(score_ref[...])
    shares = scores / jnp.sum(scores, axis=0, keepdims=True) * prob_ref[...]
    place_line = lax.broadcasted_iota(jnp.int32, (128, seqs), 0)
    table = jnp.zeros((128, seqs), F32)
    for k in range(index.shape[0]):
        table += jnp.where(place_line == lax.rem(index[k : k + 1], 2), shares[k : k + 1], 0.0)
    shares_out[...] = lax.dot_general(
        placing, table, nt, preferred_element_type=F32, precision=lax.Precision.HIGHEST
    ).reshape(GROUPS, capacity, 128)
    placing = placing.astype(BF16)

    for z in zs:
        done.append(
            send(
                shares_out.at[z],
                shares_in.at[row],
                share_send.at[z],
                share_recv.at[row],
                {"ep": z * 2 + core},
            )
        )
    shares_in[row] = shares_out[row]
    renew(0)
    own_cut = pl.ds(pl.multiple_of(tp * width, 128), width)
    total = part + stream[:, own_cut].astype(F32)
    for j in (1, 2, 0):
        parts[j].wait_recv()
        total = total + part_in[j].astype(F32)
    mixed = total.astype(BF16)
    slots = jnp.dot(placing, mixed, preferred_element_type=F32)
    slots_out[...] = slots.reshape(GROUPS, capacity, width).astype(BF16)
    for z in zs:
        done.append(
            send(
                slots_out.at[z],
                arrived.at[tp, core, row],
                slot_send.at[z],
                slot_recv.at[row],
                {"ep": z * 2 + core},
            )
        )
    arrived[tp, core, row] = slots_out[row]

    def swap(t, z):
        done.append(
            send(
                arrived.at[t, core, z],
                arrived.at[t, core, z],
                swap_send.at[t, z],
                swap_recv.at[t, z],
                {"ep": other},
            )
        )

    def join(z):
        for t in tps:
            done.append(
                send(
                    arrived.at[tp, core, z],
                    arrived.at[tp, core, z],
                    join_send.at[t, z],
                    join_recv.at[tp, z],
                    {"tp": t},
                )
            )
        swap(tp, z)

    def relay(z):
        for t in (tps[1], tps[2], tps[0]):
            expect(arrived.at[t, core, z], join_recv.at[t, z])
            swap(t, z)

    order = [row] + zs[::-1]
    join(row)
    renew(1)
    expect(arrived.at[tp, core, order[1]], slot_recv.at[order[1]])
    join(order[1])
    expect(arrived.at[tp, core, order[2]], slot_recv.at[order[2]])
    join(order[2])
    relay(order[0])
    expect(arrived.at[tp, core, order[3]], slot_recv.at[order[3]])
    join(order[3])
    renew(2)
    relay(order[1])
    relay(order[2])
    for load in expert_loads:
        load.wait()

    tokens_held = n * capacity
    square = jnp.zeros((tokens_held, 1), F32)
    before = jnp.zeros((tokens_held, 2 * inner), F32)
    for j, t in enumerate([tp, tps[1], tps[2], tps[0]]):
        if j == 1:
            relay(order[3])
        for z in order:
            expect(arrived.at[t, 1 - core, z], swap_recv.at[t, z])
        cut = pl.ds(pl.multiple_of(t * width, 128), width)
        tokens = arrived[t].astype(F32).reshape(tokens_held, width)
        square += jnp.sum(tokens * tokens, axis=-1, keepdims=True)
        scaled = (tokens * gain_ref[:, cut]).astype(BF16)
        before += lax.dot_general(
            scaled, w_in[:, :, cut].reshape(2 * inner, width), nt, preferred_element_type=F32
        )
    scale = lax.rsqrt(square / (m * width) + epsilon)
    gate_pre = before[:, :inner] * scale
    up_pre = before[:, inner:] * scale
    hidden_out[...] = (
        (gate_pre / (1.0 + jnp.exp(-gate_pre)) * up_pre).astype(BF16).reshape(2, half, inner)
    )
    for j, t in enumerate(tps):
        for c in range(2):
            done.append(
                send(
                    hidden_out.at[c],
                    hidden_in.at[core, tp],
                    hid_send.at[2 * j + c],
                    hid_recv.at[core, tp],
                    {"tp": t, "ep": row * 2 + c},
                )
            )
    done.append(
        send(
            hidden_out.at[1 - core],
            hidden_in.at[core, tp],
            hid_send.at[2 * m - 2],
            hid_recv.at[core, tp],
            {"ep": other},
        )
    )
    hidden_in[core, tp] = hidden_out[core]
    renew(3)
    pushes[4].wait_recv()
    own_sum = jnp.zeros((half, width), F32)
    pair_sum = jnp.zeros((half, width), F32)
    for j, t in enumerate([tp, tps[1], tps[2], tps[0]]):
        band = pl.ds(pl.multiple_of(t * inner, 128), inner)
        if j > 0:
            expect(hidden_in.at[core, t], hid_recv.at[core, t])
        own_sum += jnp.dot(hidden_in[core, t], w_down[0, band, :], preferred_element_type=F32)
        expect(hidden_in.at[1 - core, t], hid_recv.at[1 - core, t])
        pair_sum += jnp.dot(hidden_in[1 - core, t], pair_down[band, :], preferred_element_type=F32)
    for z in zs:
        expect(shares_in.at[z], share_recv.at[z])
    share = shares_in[...].reshape(half, 128)
    which = lax.broadcasted_iota(jnp.int32, (half, 128), 1)
    own_share = jnp.sum(jnp.where(which == core, share, 0.0), axis=1, keepdims=True)
    pair_share = jnp.sum(jnp.where(which == 1 - core, share, 0.0), axis=1, keepdims=True)
    outputs = own_share * own_sum.astype(BF16).astype(F32) + pair_share * pair_sum.astype(
        BF16
    ).astype(F32)
    ready[...] = outputs.reshape(rows, capacity, width).astype(BF16)
    for z in zs:
        done.append(
            send(
                ready.at[z],
                returned.at[row],
                back_send.at[z],
                back_recv.at[row],
                {"ep": z * 2 + core},
            )
        )
    returned[row] = ready[row]
    for z in zs[::-1]:
        expect(returned.at[z], back_recv.at[z])
    mixture = lax.dot_general(
        placing,
        returned[...].reshape(half, width),
        (((0,), (0,)), ((), ())),
        preferred_element_type=F32,
    )
    out_ref[...] = (mixed.astype(F32) + mixture).astype(BF16)
    for copy in parts + done + pushes:
        copy.wait_send()
    for b in range(3):
        middle_copy(b).wait_send()


def fused(
    stream,
    previous_state,
    mixer_norm_gain,
    query_matrix,
    key_matrix,
    value_matrix,
    output_gate_weight,
    decay_lower_factor,
    decay_upper_factor,
    forgetting_boost,
    head_norm_gain,
    output_matrix,
    mixture_norm_gain,
    expert_gate_weight,
    expert_up_weight,
    expert_down_weight,
    expert_index_table,
    expert_scores_within,
    group_probability,
):
    n = lax.axis_size("ep")
    m = lax.axis_size("tp")
    seqs, model = stream.shape
    width = previous_state.shape[2]
    span = width // DV * KEY_CHANNELS
    feats = query_matrix.shape[0]
    rank = decay_lower_factor.shape[1]
    steps = seqs // STEP
    total = 2 * span + 2 * width
    rows = n // 2
    inner = expert_gate_weight.shape[1]
    capacity = 2 * seqs * expert_index_table.shape[1] // n
    lines = 8 * STEP
    dma = pltpu.SemaphoreType.DMA
    vmem = pl.BlockSpec(memory_space=pltpu.VMEM)
    hbm = pl.BlockSpec(memory_space=pltpu.HBM)
    operands = (
        stream,
        mixer_norm_gain.reshape(1, model),
        query_matrix,
        key_matrix,
        value_matrix,
        output_gate_weight,
        decay_lower_factor.T,
        decay_upper_factor,
        forgetting_boost,
        head_norm_gain.reshape(1, DV),
        mixture_norm_gain.reshape(1, model),
        expert_index_table.T,
        expert_scores_within.T,
        group_probability.reshape(1, seqs),
        previous_state,
        output_matrix,
        expert_gate_weight,
        expert_up_weight,
        expert_down_weight,
    )
    new_state, new_stream = pl.pallas_call(
        functools.partial(layer_kernel, n, m),
        name="layer",
        out_shape=(
            pltpu.VMEM(previous_state.shape, F32),
            jax.ShapeDtypeStruct((seqs, width), BF16),
        ),
        in_specs=[hbm] * len(operands),
        out_specs=(vmem, vmem),
        scratch_shapes=[
            pltpu.VMEM((seqs, model), BF16),
            pltpu.VMEM((1, model), F32),
            pltpu.VMEM((2 * feats, total), BF16),
            pltpu.VMEM((rank, model), BF16),
            pltpu.VMEM((rank, span), BF16),
            pltpu.VMEM((seqs, span), F32),
            pltpu.VMEM((1, DV), F32),
            pltpu.VMEM((1, model), F32),
            pltpu.VMEM(expert_index_table.shape[::-1], jnp.int32),
            pltpu.VMEM(expert_scores_within.shape[::-1], F32),
            pltpu.VMEM((1, seqs), F32),
            pltpu.VMEM(output_matrix.shape, BF16),
            pltpu.VMEM((2, *expert_gate_weight.shape[1:]), BF16),
            pltpu.VMEM(expert_down_weight.shape, BF16),
            pltpu.VMEM(expert_down_weight.shape[1:], BF16),
            pltpu.VMEM((rows, seqs, 2 * feats), BF16),
            pltpu.VMEM((rows, seqs, 2 * feats), BF16),
            pltpu.VMEM((seqs, total), BF16),
            pltpu.VMEM((seqs, total), BF16),
            pltpu.VMEM((seqs, total), BF16),
            pltpu.VMEM((seqs, total), BF16),
            pltpu.VMEM((seqs, total), BF16),
            pltpu.VMEM((2, seqs, total), BF16),
            pltpu.VMEM((seqs, total), F32),
            pltpu.VMEM((steps, lines, span), F32),
            pltpu.VMEM((steps, width // DV, KEY_CHANNELS, lines), BF16),
            pltpu.VMEM((lines, 3 * STEP * KEY_CHANNELS), BF16),
            pltpu.VMEM((width // DV, KEY_CHANNELS, 2 * STEP * KEY_CHANNELS), F32),
            pltpu.VMEM((seqs, width), F32),
            pltpu.VMEM((seqs, 8, width), F32),
            pltpu.VMEM((m - 1, seqs, width), BF16),
            pltpu.VMEM((m - 1, seqs, width), BF16),
            pltpu.VMEM((GROUPS, capacity, width), BF16),
            pltpu.VMEM((GROUPS, capacity, 128), F32),
            pltpu.VMEM((GROUPS, capacity, 128), F32),
            pltpu.VMEM((m, 2, rows, capacity, width), BF16),
            pltpu.VMEM((2, rows * capacity, inner), BF16),
            pltpu.VMEM((2, m, rows * capacity, inner), BF16),
            pltpu.VMEM((rows, capacity, width), BF16),
            pltpu.VMEM((rows, capacity, width), BF16),
            dma((len(operands),)),
            dma((5,)),
            dma((5,)),
            dma((rows,)),
            dma((rows,)),
            dma((3,)),
            dma((3,)),
            dma((3,)),
            dma((3,)),
            dma((3,)),
            dma((2, 3)),
            dma((m - 1,)),
            dma((m - 1,)),
            dma((rows,)),
            dma((rows,)),
            dma((rows,)),
            dma((rows,)),
            dma((m, rows)),
            dma((m, rows)),
            dma((m, rows)),
            dma((m, rows)),
            dma((2 * m - 1,)),
            dma((2, m)),
            dma((rows,)),
            dma((rows,)),
        ],
        compiler_params=pltpu.CompilerParams(
            collective_id=0, has_side_effects=True, vmem_limit_bytes=GRANT * 2**20
        ),
        cost_estimate=pl.CostEstimate(
            flops=COST, bytes_accessed=4 * previous_state.size, transcendentals=0
        ),
    )(*(pltpu.with_memory_space_constraint(a, pltpu.HBM) for a in operands))
    return (new_stream, new_state)


def on_device(*arrays):
    stream, state = arrays[0], arrays[1]
    experts_held, route_count = arrays[13].shape[0], arrays[16].shape[1]
    n = lax.axis_size("ep")
    whole_heads = state.shape[2] % DV == 0
    pair_routed = experts_held == 1 and n == GROUPS * route_count and route_count == 2
    boxed = n == 8 and lax.axis_size("tp") == 4
    full_tiles = stream.shape[0] % 16 == 0 and stream.shape[1] == state.shape[2] * lax.axis_size("tp")
    if whole_heads and pair_routed and full_tiles and boxed:
        return fused(*arrays)
    return general(*arrays)


def solution(mesh):
    placed = (
        P("ep", None),
        P("ep", None, "tp"),
        P(),
        P("ep", None),
        P("ep", None),
        P("ep", "tp"),
        P("ep", "tp"),
        P(),
        P(),
        P("ep", None),
        P(),
        P("tp", None),
        P(),
        P("ep", "tp", None),
        P("ep", "tp", None),
        P("ep", None, "tp"),
        P("ep", None),
        P("ep", None),
        P("ep"),
    )
    return jax.shard_map(
        on_device,
        mesh=mesh,
        in_specs=placed,
        out_specs=(P("ep", "tp"), P("ep", None, "tp")),
        check_vma=False,
    )
```
